32 devices in a mesh: sp: 16 (over z, y, x), tp: 2 (over core).
Axes of the slice: x: 2, y: 2, z: 4, core: 2. Of those that a mesh axis runs over, the one named last changes fastest.
Arguments:
- tokens: bfloat16 [2048, 2048], P('sp', 'tp'), may hold values from -6 to 6
- pre_gain: float32 [2048], replicated, may hold values from 0.1 to 1.9
- w_query_stick: bfloat16 [2048, 1024], P(None, 'tp'), may hold values from -0.125 to 0.125
- w_key_stick: bfloat16 [2048, 1024], P(None, 'tp'), may hold values from -0.125 to 0.125
- w_value_stick: bfloat16 [2048, 1024], P(None, 'tp'), may hold values from -2 to 2, as said below
- w_query_window: bfloat16 [2048, 1024], P(None, 'tp'), may hold values from -20 to 20, as said below
- w_key_window: bfloat16 [2048, 512], P(None, 'tp'), may hold values from -1 to 1, as said below
- w_value_window: bfloat16 [2048, 512], P(None, 'tp'), may hold values from -2 to 2, as said below
- stick_bias: float32 [16], P('tp'), may hold values from -14 to -3
- sinks: float32 [16], P('tp'), may hold values from 2 to 6
- stick_gain: float32 [1024], P('tp'), may hold values from 0.1 to 1.9
- window_gain: float32 [1024], P('tp'), may hold values from 0.1 to 1.9
- w_out_stick: bfloat16 [1024, 2048], P('tp'), may hold values from -0.125 to 0.125
- w_out_window: bfloat16 [1024, 2048], P('tp'), may hold values from -0.125 to 0.125
- post_gain: float32 [2048], replicated, may hold values from 0.1 to 1.9
Outputs:
- layer_out: bfloat16 [2048, 2048], P(('sp', 'tp'))
The draws below stay inside these ranges and needn't reach their ends.
Inputs may be any that keep to these rules, and one draw needn't show every extreme that they name: `w_key_window`: key weights of the windowed heads. `w_query_window`: query weights of the windowed heads. `w_value_stick`: value weights of the stick-breaking heads. `w_value_window`: value weights of the windowed heads.
All inputs are finite; a program needn't handle non-finite values.
Results may differ from the reference program's by a relative error of at most 0.018.
Values may be sent and summed in bfloat16 or wider, within the bound.
A program may use at most 64 MiB of HBM per device.

```python
import jax
import jax.numpy as jnp
from jax import lax

D = 2048
HEAD_DIM = 64
SB_HEADS = 16
SW_KV_HEADS = 8
GROUP = 2
WINDOW = 128
TOK_DEV = 128
TOKENS = 2048
SW_HEADS = 16
SB_WIDTH = 1024
SW_WIDTH = 1024


def clipped_normal(key, shape):
    return jnp.clip(jax.random.normal(key, shape, jnp.float32), -4.0, 4.0)


def window_pair(key):
    salted = jax.random.fold_in(key, 17)
    keys_w = clipped_normal(jax.random.fold_in(salted, 1), (D, SW_KV_HEADS * HEAD_DIM)) * D ** (-0.5)
    queries_w = clipped_normal(jax.random.fold_in(salted, 2), (D, SW_HEADS * HEAD_DIM)) * D ** (-0.5)
    return (keys_w, queries_w)


def draw_w_key_window(key, part):
    return window_pair(key)[0].astype(jnp.bfloat16)


def draw_w_query_window(key, part):
    keys_w, queries_w = window_pair(key)
    return queries_w.astype(jnp.bfloat16)


def scaled_values(key, salt, head_count):
    salted = jax.random.fold_in(key, salt)
    head_scale = jnp.exp(jax.random.uniform(jax.random.fold_in(salted, 1), (head_count,), jnp.float32, -1.2, 1.2))
    normals = clipped_normal(jax.random.fold_in(salted, 2), (D, head_count * HEAD_DIM)) * D ** (-0.5)
    return normals * jnp.repeat(head_scale, HEAD_DIM)[None, :]


def draw_w_value_stick(key, part):
    return scaled_values(key, 23, SB_HEADS).astype(jnp.bfloat16)


def draw_w_value_window(key, part):
    return scaled_values(key, 31, SW_KV_HEADS).astype(jnp.bfloat16)


def draw_stick_bias(key, part):
    salted = jax.random.fold_in(key, 29)
    slow_bias = -jnp.log(TOKENS * 1.0) - jax.random.uniform(jax.random.fold_in(salted, 1), (SB_HEADS,), jnp.float32, 0.0, 1.0)
    fast_bias = jax.random.uniform(jax.random.fold_in(salted, 2), (SB_HEADS,), jnp.float32, -4.0, -3.5)
    chosen = jax.random.permutation(jax.random.fold_in(salted, 3), SB_HEADS) < SB_HEADS // 2
    return jnp.where(chosen, slow_bias, fast_bias)


def steps_of(own_key, shape, split, smallest, high):
    def one(position, blocks):
        heights = jax.random.uniform(jax.random.fold_in(jax.random.fold_in(own_key, 6), position), (blocks,), jnp.float32, smallest / len(split), high / len(split))
        return jnp.repeat(jnp.exp(heights), shape[position] // blocks).reshape((-1,) + (1,) * (len(shape) - position - 1))

    level = one(*split[0])
    for cut in split[1:]:
        level = level * one(*cut)
    return level


def scatter_about(own_key, shape, width, most, split=(), held_as=jnp.bfloat16):
    values = width * jax.random.normal(own_key, shape, jnp.float32)
    if split:
        values = values * steps_of(own_key, shape, split, -0.22, 0.18)
    return jnp.clip(values, -most, most).astype(held_as)


def setup_inputs(seed: int = 0) -> dict:
    key_of = jax.random.split(jax.random.key(seed), 16)
    return {
        "tokens": scatter_about(key_of[0], (TOKENS, D), 1.0, 6.0, ((0, 16), (1, 2))),
        "pre_gain": jnp.clip(1.0 + 0.18 * jax.random.normal(key_of[1], (D,), jnp.float32), 0.1, 1.9),
        "w_query_stick": scatter_about(key_of[2], (D, SB_WIDTH), D ** -0.5, 0.125, ((1, 2),)),
        "w_key_stick": scatter_about(key_of[3], (D, SB_WIDTH), D ** -0.5, 0.125, ((1, 2),)),
        "w_value_stick": draw_w_value_stick(jax.random.fold_in(key_of[15], 71), 0),
        "w_query_window": draw_w_query_window(jax.random.fold_in(key_of[15], 71), 0),
        "w_key_window": draw_w_key_window(jax.random.fold_in(key_of[15], 71), 0),
        "w_value_window": draw_w_value_window(jax.random.fold_in(key_of[15], 71), 0),
        "stick_bias": draw_stick_bias(jax.random.fold_in(key_of[15], 71), 0),
        "sinks": jnp.clip(2.0 + 4.0 * jax.random.uniform(key_of[9], (SW_HEADS,), jnp.float32) ** steps_of(key_of[9], (SW_HEADS,), ((0, 2),), -0.2, 0.2), 2.0, 6.0),
        "stick_gain": jnp.clip(1.0 + 0.18 * jax.random.normal(key_of[10], (SB_WIDTH,), jnp.float32), 0.1, 1.9),
        "window_gain": jnp.clip(1.0 + 0.18 * jax.random.normal(key_of[11], (SW_WIDTH,), jnp.float32), 0.1, 1.9),
        "w_out_stick": scatter_about(key_of[12], (SB_WIDTH, D), (SB_WIDTH + SW_WIDTH) ** -0.5, 0.125, ((0, 2),)),
        "w_out_window": scatter_about(key_of[13], (SW_WIDTH, D), (SB_WIDTH + SW_WIDTH) ** -0.5, 0.125, ((0, 2),)),
        "post_gain": jnp.clip(1.0 + 0.18 * jax.random.normal(key_of[14], (D,), jnp.float32), 0.1, 1.9),
    }


epsilon = 1e-06

def rounded(values):
    return lax.optimization_barrier(values.astype(jnp.bfloat16)).astype(jnp.float32)

def norm_rows(values, gain):
    stats = lax.optimization_barrier(jnp.mean(values * values, axis=-1, keepdims=True))
    return values * lax.rsqrt(stats + epsilon) * gain

def stick_attention(queries, key_rows, values, stick_bias):
    blocks = TOKENS // TOK_DEV
    q_blocks = queries.reshape(blocks, TOK_DEV, SB_HEADS, HEAD_DIM).astype(jnp.float32)
    k_blocks = key_rows.reshape(blocks, TOK_DEV, SB_HEADS, HEAD_DIM).astype(jnp.float32)
    v_blocks = values.reshape(blocks, TOK_DEV, SB_HEADS, HEAD_DIM).astype(jnp.float32)
    offsets = jnp.arange(TOK_DEV, dtype=jnp.int32)
    scaling = HEAD_DIM ** (-0.5)

    def one_query(block_args):
        q_blk, q_index = block_args
        q_pos = q_index * TOK_DEV + offsets

        def key_step(carried, inputs):
            result, logsum = carried
            k_blk, v_blk, k_index = inputs
            k_pos = k_index * TOK_DEV + offsets
            before = (k_pos[None, :] < q_pos[:, None])[None]
            scores = jnp.einsum('thd,shd->hts', q_blk, k_blk) * scaling + stick_bias[:, None, None]
            log_keep = jnp.where(before, jax.nn.log_sigmoid(-scores), 0.0)
            suffix = lax.cumsum(log_keep, axis=2, reverse=True) - log_keep
            stick_weights = jnp.where(before, jnp.exp(jax.nn.log_sigmoid(scores) + suffix + logsum[:, :, None]), 0.0)
            stick_weights = rounded(stick_weights)
            result = result + jnp.einsum('hts,shd->htd', stick_weights, v_blk)
            logsum = logsum + lax.optimization_barrier(jnp.sum(log_keep, axis=2))
            return ((result, logsum), None)
        initial = (jnp.zeros((SB_HEADS, TOK_DEV, HEAD_DIM), jnp.float32), jnp.zeros((SB_HEADS, TOK_DEV), jnp.float32))
        (result, _), _ = lax.scan(key_step, initial, (k_blocks, v_blocks, jnp.arange(blocks, dtype=jnp.int32)), reverse=True)
        return result.transpose(1, 0, 2)
    outputs = lax.map(one_query, (q_blocks, jnp.arange(blocks, dtype=jnp.int32)))
    return outputs.reshape(TOKENS, SB_WIDTH).astype(jnp.bfloat16)

def window_attention(queries, key_rows, values, sinks):
    block_count = TOKENS // WINDOW
    q_blocks = queries.reshape(block_count, WINDOW, SW_KV_HEADS, GROUP, HEAD_DIM).astype(jnp.float32)
    k_heads = key_rows.reshape(block_count, WINDOW, SW_KV_HEADS, HEAD_DIM).astype(jnp.float32)
    v_heads = values.reshape(block_count, WINDOW, SW_KV_HEADS, HEAD_DIM).astype(jnp.float32)
    zero_block = jnp.zeros((1, WINDOW, SW_KV_HEADS, HEAD_DIM), jnp.float32)
    k_band = jnp.concatenate([jnp.concatenate([zero_block, k_heads[:-1]], axis=0), k_heads], axis=1)
    v_band = jnp.concatenate([jnp.concatenate([zero_block, v_heads[:-1]], axis=0), v_heads], axis=1)
    logits = jnp.einsum('nqhgd,nchd->nhgqc', q_blocks, k_band) * HEAD_DIM ** (-0.5)
    query_offs = jnp.arange(WINDOW, dtype=jnp.int32)[:, None]
    key_offs = jnp.arange(2 * WINDOW, dtype=jnp.int32)[None, :]
    distance = query_offs + WINDOW - key_offs
    key_pos = jnp.arange(block_count, dtype=jnp.int32)[:, None] * WINDOW - WINDOW + key_offs
    usable = ((distance >= 0) & (distance < WINDOW))[None] & (key_pos >= 0)[:, None, :]
    logits = jnp.where(usable[:, None, None], logits, -jnp.inf)
    sink_logit = sinks.reshape(SW_KV_HEADS, GROUP)[None, :, :, None, None]
    row_top = jnp.maximum(lax.optimization_barrier(jnp.max(logits, axis=-1, keepdims=True)), sink_logit)
    weights_exp = jnp.exp(logits - row_top)
    normalizer = lax.optimization_barrier(jnp.sum(weights_exp, axis=-1, keepdims=True)) + jnp.exp(sink_logit - row_top)
    window_weights = rounded(weights_exp / normalizer)
    result = jnp.einsum('nhgqc,nchd->nqhgd', window_weights, v_band)
    return result.reshape(TOKENS, SW_WIDTH).astype(jnp.bfloat16)

def reference(tokens, pre_gain, w_query_stick, w_key_stick, w_value_stick, w_query_window, w_key_window, w_value_window, stick_bias, sinks, stick_gain, window_gain, w_out_stick, w_out_window, post_gain):
    normed = norm_rows(tokens.astype(jnp.float32), pre_gain).astype(jnp.bfloat16)

    def project(weight):
        return jnp.dot(normed, weight, preferred_element_type=jnp.float32).astype(jnp.bfloat16)
    stick_out = stick_attention(project(w_query_stick), project(w_key_stick), project(w_value_stick), stick_bias)
    window_out = window_attention(project(w_query_window), project(w_key_window), project(w_value_window), sinks)
    stick_normed = norm_rows(stick_out.astype(jnp.float32), stick_gain).astype(jnp.bfloat16)
    window_normed = norm_rows(window_out.astype(jnp.float32), window_gain).astype(jnp.bfloat16)
    combined = jnp.dot(stick_normed, w_out_stick, preferred_element_type=jnp.float32)
    combined = combined + jnp.dot(window_normed, w_out_window, preferred_element_type=jnp.float32)
    combined = rounded(combined)
    return norm_rows(combined, post_gain).astype(jnp.bfloat16)
```

```python
import functools

import jax
import jax.numpy as jnp
from jax import lax
from jax.experimental import pallas as pl
from jax.experimental.pallas import tpu as pltpu
from jax.sharding import PartitionSpec as P

HEAD_DIM = 64
GROUP = 2
WINDOW = 128
EPS = 1e-06
LOG2E = 1.4426950408889634
MESH = pl.DeviceIdType.MESH


def dot(a, b):
    return jnp.dot(a, b, preferred_element_type=jnp.float32)


def dot_t(a, b):
    return lax.dot_general(a, b, (((1,), (1,)), ((), ())), preferred_element_type=jnp.float32)


def kernel(
    n_sp,
    tokens, pre_gain, wqs, wks, wvs, wqw, wkw, wvw, bias, sinks, sgain, wgain, wos, wow, post_gain,
    out,
    x, bias_buf, normed, vqs, vks, vvs, vqw, vkw, vvw, vos, vow,
    kv_send, q_send, kv_all, q_all, q_pad, staged,
    kvw, kvw_prev, w_out_buf, o_send, o_recv, s_out_buf,
    sq_send, sq_recv, total_w, comb, c_send, c_recv,
    w_sem, tok_sem, x_ss, x_rs, b_ss, b_rs, kv_ss, kv_rs, q_ss, q_rs, f_ss, f_rs,
    p_ss, p_rs, o_ss, o_rs, sq_ss, sq_rs, c_ss, c_rs,
):
    bf = jnp.bfloat16
    f32 = jnp.float32
    s = lax.axis_index("sp")
    t = lax.axis_index("tp")
    other = 1 - t
    rows, feat_half = tokens.shape
    feats = 2 * feat_half
    half = rows // 2
    quarter = half // 2
    hd = HEAD_DIM
    heads = wqs.shape[1] // hd
    kv_heads = wkw.shape[1] // hd
    sw = wqs.shape[1]

    loads = [
        pltpu.make_async_copy(src, dst, w_sem.at[n])
        for n, (src, dst) in enumerate(
            [(wks, vks), (wvs, vvs), (wqs, vqs), (wkw, vkw), (wvw, vvw), (wqw, vqw), (wow, vow), (wos, vos)]
        )
    ]
    l_ks, l_vs, l_qs, l_kw, l_vw, l_qw, l_ow, l_os = loads
    tok_load = pltpu.make_async_copy(tokens, x.at[t], tok_sem)
    tok_load.start()
    for load in loads:
        load.start()

    row_id = lax.broadcasted_iota(jnp.int32, (heads, 128), 0)
    bias_rows = jnp.zeros((heads, 128), f32)
    for i in range(heads):
        bias_rows = jnp.where(row_id == i, bias[i] * LOG2E, bias_rows)
    bias_buf[t] = bias_rows

    barrier = pltpu.get_barrier_semaphore()
    me = s * 2 + t

    def greet(k, carry):
        peer = lax.rem(me + k, 2 * n_sp)
        pl.semaphore_signal(
            barrier, inc=1, device_id={"sp": peer // 2, "tp": lax.rem(peer, 2)}, device_id_type=MESH
        )
        return carry

    lax.fori_loop(1, 2 * n_sp, greet, 0)
    tok_load.wait()
    pl.semaphore_wait(barrier, 2 * n_sp - 1)

    def to_partner(src, dst, ss, rs):
        return pltpu.make_async_remote_copy(
            src_ref=src, dst_ref=dst, send_sem=ss, recv_sem=rs,
            device_id={"sp": s, "tp": other}, device_id_type=MESH,
        )

    x_copy = to_partner(x.at[t], x.at[t], x_ss, x_rs)
    b_copy = to_partner(bias_buf.at[t], bias_buf.at[t], b_ss, b_rs)
    x_copy.start()
    b_copy.start()
    x_copy.wait_recv()

    gain = pre_gain[...].reshape(1, feats)

    def norm_step(n, carry):
        part = pl.ds(pl.multiple_of(n * 32, 32), 32)
        left = x[0, part, :].astype(f32)
        right = x[1, part, :].astype(f32)
        stats = (
            jnp.sum(left * left, axis=1, keepdims=True) + jnp.sum(right * right, axis=1, keepdims=True)
        ) * (1.0 / feats)
        inv = lax.rsqrt(stats + EPS)
        normed[part, :feat_half] = (left * inv * gain[:, :feat_half]).astype(bf)
        normed[part, feat_half:] = (right * inv * gain[:, feat_half:]).astype(bf)
        return carry

    lax.fori_loop(0, rows // 32, norm_step, 0)

    l_ks.wait()
    keys = dot(normed[...], vks[...])
    l_vs.wait()
    values = dot(normed[...], vvs[...])
    for i in range(heads):
        cols = slice(i * hd, (i + 1) * hd)
        packed = jnp.concatenate([keys[:, cols], values[:, cols]], axis=1).astype(bf)
        kv_send[i] = packed.reshape(2, half, 2 * hd)

    def scatter(send, slots, ss, rs):
        def step(k, carry):
            i = lax.rem(k // 2 + s, heads)
            u = lax.rem(k, 2)
            chip = t * heads + i
            is_self = jnp.logical_and(chip == s, u == t)

            @pl.when(is_self)
            def _():
                pltpu.make_async_copy(send.at[i, u], slots(u), rs.at[s]).start()

            @pl.when(jnp.logical_not(is_self))
            def _():
                pltpu.make_async_remote_copy(
                    src_ref=send.at[i, u], dst_ref=slots(u), send_sem=ss.at[i, u], recv_sem=rs.at[s],
                    device_id={"sp": chip, "tp": u}, device_id_type=MESH,
                ).start()

            return carry

        lax.fori_loop(0, 2 * heads, step, 0)

    def scatter_done(send, slots, ss, rs):
        def step(k, carry):
            i = k // 2
            u = lax.rem(k, 2)
            chip = t * heads + i
            is_self = jnp.logical_and(chip == s, u == t)

            @pl.when(jnp.logical_not(is_self))
            def _():
                pltpu.make_async_remote_copy(
                    src_ref=send.at[i, u], dst_ref=slots(u), send_sem=ss.at[i, u], recv_sem=rs.at[s],
                    device_id={"sp": chip, "tp": u}, device_id_type=MESH,
                ).wait_send()

            return carry

        lax.fori_loop(0, 2 * heads, step, 0)

    kv_slot = lambda u: kv_all.at[s, u]
    q_slot = lambda u: q_all.at[s]
    scatter(kv_send, kv_slot, kv_ss, kv_rs)

    l_qs.wait()
    queries = dot(normed[...], vqs[...])
    for i in range(heads):
        cols = slice(i * hd, (i + 1) * hd)
        for u in range(2):
            top = queries[u * half : u * half + quarter, cols]
            low = queries[u * half + quarter : (u + 1) * half, cols]
            q_send[i, u] = jnp.concatenate([top, low], axis=1).astype(bf)
    scatter(q_send, q_slot, q_ss, q_rs)

    l_kw.wait()
    kvw[:, : kv_heads * hd] = dot(normed[...], vkw[...]).astype(bf)
    l_vw.wait()
    kvw[:, kv_heads * hd :] = dot(normed[...], vvw[...]).astype(bf)
    prev_copy = lambda to: pltpu.make_async_remote_copy(
        src_ref=kvw, dst_ref=kvw_prev, send_sem=p_ss, recv_sem=p_rs,
        device_id={"sp": to, "tp": t}, device_id_type=MESH,
    )

    @pl.when(s < n_sp - 1)
    def _():
        prev_copy(s + 1).start()

    l_qw.wait()
    qw = dot(normed[...], vqw[...])

    @pl.when(s == 0)
    def _():
        kvw_prev[...] = jnp.zeros_like(kvw_prev)

    @pl.when(s > 0)
    def _():
        prev_copy(s - 1).wait_recv()

    def forward(k, carry):
        src = n_sp - 1 - k
        pltpu.make_async_remote_copy(
            src_ref=kv_send.at[0, 0], dst_ref=kv_all.at[src, t], send_sem=kv_ss.at[0, 0],
            recv_sem=kv_rs.at[src], device_id={"sp": s, "tp": other}, device_id_type=MESH,
        ).wait_recv()
        to_partner(kv_all.at[src, t], kv_all.at[src, t], f_ss.at[src], f_rs.at[src]).start()
        return carry

    def forward_arrived(k, carry):
        to_partner(kv_all.at[k, other], kv_all.at[k, other], f_ss.at[k], f_rs.at[k]).wait_recv()
        return carry

    def forward_sent(k, carry):
        to_partner(kv_all.at[k, t], kv_all.at[k, t], f_ss.at[k], f_rs.at[k]).wait_send()
        return carry

    two = 2 * rows
    r_iota = lax.broadcasted_iota(jnp.int32, (two, two), 0)
    c_iota = lax.broadcasted_iota(jnp.int32, (two, two), 1)
    dist = lax.rem(r_iota, rows) + rows - c_iota
    in_window = (dist >= 0) & (dist < WINDOW) & ((c_iota >= rows) | (s > 0))
    first_rows = lax.broadcasted_iota(jnp.int32, (two, 1), 0) < rows
    for g in range(kv_heads):
        cols = slice(g * hd, (g + 1) * hd)
        v_cols = slice((kv_heads + g) * hd, (kv_heads + g + 1) * hd)
        kk = jnp.concatenate([kvw_prev[:, cols], kvw[:, cols]], axis=0)
        vv = jnp.concatenate([kvw_prev[:, v_cols], kvw[:, v_cols]], axis=0)
        base = g * GROUP * hd
        qq = jnp.concatenate(
            [qw[:, base : base + hd], qw[:, base + hd : base + 2 * hd]], axis=0
        ).astype(bf)
        logits = jnp.where(in_window, dot_t(qq, kk) * hd**-0.5, -jnp.inf)
        sink = jnp.where(first_rows, sinks[GROUP * g], sinks[GROUP * g + 1])
        top = jnp.maximum(jnp.max(logits, axis=1, keepdims=True), sink)
        grown = jnp.exp(logits - top)
        total = jnp.sum(grown, axis=1, keepdims=True) + jnp.exp(sink - top)
        weights = (grown / total).astype(bf)
        res = dot(weights, vv)
        w_out_buf[:, base : base + 2 * hd] = jnp.concatenate([res[:rows], res[rows:]], axis=1).astype(bf)

    wf = w_out_buf[...].astype(f32)
    sq_send[0] = jnp.broadcast_to(jnp.sum(wf * wf, axis=1, keepdims=True), (rows, 128))

    lax.fori_loop(0, n_sp, forward, 0)
    sq_w = to_partner(sq_send.at[0], sq_recv.at[0], sq_ss.at[0], sq_rs.at[0])
    sq_w.start()

    def take_q(k, carry):
        pltpu.make_async_remote_copy(
            src_ref=q_send.at[0, 0], dst_ref=q_all.at[k], send_sem=q_ss.at[0, 0],
            recv_sem=q_rs.at[k], device_id={"sp": s, "tp": other}, device_id_type=MESH,
        ).wait_recv()
        slab = q_all[k].astype(f32)
        zero = jnp.zeros((quarter, hd), f32)
        both = jnp.concatenate(
            [
                jnp.concatenate([slab[:, :hd], zero], axis=1),
                jnp.concatenate([slab[:, hd:], zero], axis=1),
            ],
            axis=0,
        )
        q_pad[pl.ds(pl.multiple_of(k * half, half), half), :] = both.astype(bf)
        return carry

    lax.fori_loop(0, n_sp, take_q, 0)
    lax.fori_loop(0, n_sp, forward_arrived, 0)
    b_copy.wait_recv()
    head_bias = bias_buf[s // heads, pl.ds(lax.rem(s, heads), 1), :][:, :1]

    kt = 2 * rows
    chunk = 4 * half
    later = (
        lax.broadcasted_iota(jnp.int32, (kt, kt), 0) > lax.broadcasted_iota(jnp.int32, (kt, kt), 1)
    ).astype(bf)
    row = lax.broadcasted_iota(jnp.int32, (chunk, kt), 0)
    lane = lax.broadcasted_iota(jnp.int32, (chunk, kt), 1)
    q_at = (row // half) * rows + t * half + lax.rem(row, half)
    scale = LOG2E * hd**-0.5

    def tile_of(n):
        return kv_all[2 * n : 2 * n + 2].reshape(kt, 2 * hd)

    owner = s // heads
    slot = lax.rem(s, heads)
    for qc in reversed(range(n_sp // 4)):
        last = 2 * qc + 1
        carry = jnp.zeros((chunk, 1), f32)
        carries = {}
        for n in range(last, -1, -1):
            low = chunk // 2 if n == last else 0
            qs = q_pad[qc * chunk + low : (qc + 1) * chunk, :]
            z = dot_t(qs, tile_of(n)) * scale + head_bias
            pos = jnp.maximum(z, 0.0)
            neg = z - pos
            soft = jnp.log2(1.0 + jnp.exp2(neg - pos))
            drop = pos + soft
            hold = neg - soft
            if n >= last - 1:
                usable = (lane + (n - 2 * qc) * kt < q_at)[low:]
                drop = jnp.where(usable, drop, 0.0)
                hold = jnp.where(usable, hold, -jnp.inf)
            suffix = dot(drop.astype(bf), later)
            staged[low:, n * kt : (n + 1) * kt] = hold - suffix
            carries[n] = carry[low:]
            step = suffix[:, :1] + drop[:, :1]
            if low:
                step = jnp.concatenate([jnp.zeros((low, 1), f32), step], axis=0)
            carry = carry + step
        acc = None
        for n in range(last - 1, -1, -1):
            weights = jnp.exp2(staged[:, n * kt : (n + 1) * kt] - carries[n]).astype(bf)
            res = dot(weights, tile_of(n))
            acc = res if acc is None else acc + res
        low = chunk // 2
        weights = jnp.exp2(staged[low:, last * kt : (last + 1) * kt] - carries[last]).astype(bf)
        tail = dot(weights, tile_of(last))
        acc = jnp.concatenate([acc[:low], acc[low:] + tail], axis=0)
        for b in range(4):
            top = acc[b * half : b * half + quarter, hd:]
            bot = acc[b * half + quarter : (b + 1) * half, hd:]
            o_send[qc * 4 + b] = jnp.concatenate([top, bot], axis=1).astype(bf)

        def give(k, carry):
            is_self = jnp.logical_and(k == s, t == owner)

            @pl.when(is_self)
            def _():
                pltpu.make_async_copy(o_send.at[k], o_recv.at[slot, t], o_rs.at[slot, t]).start()

            @pl.when(jnp.logical_not(is_self))
            def _():
                pltpu.make_async_remote_copy(
                    src_ref=o_send.at[k], dst_ref=o_recv.at[slot, t], send_sem=o_ss.at[k],
                    recv_sem=o_rs.at[slot, t], device_id={"sp": k, "tp": owner}, device_id_type=MESH,
                ).start()

            return carry

        lax.fori_loop(qc * 4, qc * 4 + 4, give, 0)

    l_ow.wait()
    total_w[...] = dot((wf * wgain[...].reshape(1, sw)).astype(bf), vow[...])
    sq_w.wait_recv()
    sw_cols = 2.0 * sw
    inv_w = lax.rsqrt((sq_send[0] + sq_recv[0])[:, :1] / sw_cols + EPS)

    def take_o(k, carry):
        pltpu.make_async_remote_copy(
            src_ref=o_send.at[0], dst_ref=o_recv.at[k // 2, lax.rem(k, 2)], send_sem=o_ss.at[0],
            recv_sem=o_rs.at[k // 2, lax.rem(k, 2)], device_id={"sp": s, "tp": other}, device_id_type=MESH,
        ).wait_recv()
        return carry

    lax.fori_loop(0, 2 * heads, take_o, 0)
    for j in range(heads // 2):
        for u in range(2):
            one = o_recv[2 * j, u].astype(f32)
            two_ = o_recv[2 * j + 1, u].astype(f32)
            s_out_buf[u * half : u * half + quarter, 2 * j * hd : 2 * (j + 1) * hd] = jnp.concatenate(
                [one[:, :hd], two_[:, :hd]], axis=1
            )
            s_out_buf[u * half + quarter : (u + 1) * half, 2 * j * hd : 2 * (j + 1) * hd] = jnp.concatenate(
                [one[:, hd:], two_[:, hd:]], axis=1
            )
    sf = s_out_buf[...]
    sq_send[1] = jnp.broadcast_to(jnp.sum(sf * sf, axis=1, keepdims=True), (rows, 128))
    gained = (sf * sgain[...].reshape(1, sw)).astype(bf)
    sq_s = to_partner(sq_send.at[1], sq_recv.at[1], sq_ss.at[1], sq_rs.at[1])
    sq_s.start()
    l_os.wait()
    n_cut = c_send.shape[0]
    cut = feats // n_cut
    for n in range(n_cut):
        comb[:, n * cut : (n + 1) * cut] = dot(gained, vos[:, n * cut : (n + 1) * cut])
    sq_s.wait_recv()
    inv_s = lax.rsqrt((sq_send[1] + sq_recv[1])[:, :1] / sw_cols + EPS)
    copies = []
    theirs = pl.ds(pl.multiple_of(other * half, half), half)
    mine = pl.ds(pl.multiple_of(t * half, half), half)
    for n in range(n_cut):
        cols = slice(n * cut, (n + 1) * cut)
        comb[:, cols] = comb[:, cols] * inv_s + total_w[:, cols] * inv_w
        c_send[n] = comb[theirs, cols].astype(bf)
        copy = to_partner(c_send.at[n], c_recv.at[n], c_ss.at[n], c_rs.at[n])
        copy.start()
        copies.append(copy)
    square = jnp.zeros((half, 1), f32)
    for n in range(n_cut):
        cols = slice(n * cut, (n + 1) * cut)
        copies[n].wait_recv()
        summed = (comb[mine, cols] + c_recv[n].astype(f32)).astype(bf).astype(f32)
        total_w[:half, cols] = summed
        square = square + jnp.sum(summed * summed, axis=1, keepdims=True)
    inv = lax.rsqrt(square / feats + EPS)
    out[...] = (total_w[:half, :] * inv * post_gain[...].reshape(1, feats)).astype(bf)

    x_copy.wait_send()
    b_copy.wait_send()
    scatter_done(kv_send, kv_slot, kv_ss, kv_rs)
    scatter_done(q_send, q_slot, q_ss, q_rs)
    lax.fori_loop(0, n_sp, forward_sent, 0)

    @pl.when(s < n_sp - 1)
    def _():
        prev_copy(s + 1).wait_send()

    def gave(k, carry):
        @pl.when(jnp.logical_not(jnp.logical_and(k == s, t == owner)))
        def _():
            pltpu.make_async_remote_copy(
                src_ref=o_send.at[k], dst_ref=o_recv.at[slot, t], send_sem=o_ss.at[k],
                recv_sem=o_rs.at[slot, t], device_id={"sp": k, "tp": owner}, device_id_type=MESH,
            ).wait_send()

        return carry

    lax.fori_loop(0, n_sp, gave, 0)
    sq_w.wait_send()
    sq_s.wait_send()
    for copy in copies:
        copy.wait_send()


def one_kernel(n_sp, *args):
    tokens, pre_gain, wqs, wks, wvs, wqw, wkw, wvw, bias, sinks, sgain, wgain, wos, wow, post_gain = args
    bf = jnp.bfloat16
    f32 = jnp.float32
    rows, feat_half = tokens.shape
    feats = 2 * feat_half
    half = rows // 2
    hd = HEAD_DIM
    heads = wqs.shape[1] // hd
    sw = wqs.shape[1]
    wide = 2 * hd
    kvw_cols = wkw.shape[1] + wvw.shape[1]
    assert 2 * heads == n_sp and rows == WINDOW
    v = pltpu.VMEM
    dma = pltpu.SemaphoreType.DMA
    anywhere = pl.BlockSpec(memory_space=pl.ANY)
    vmem = pl.BlockSpec(memory_space=pltpu.VMEM)
    smem = pl.BlockSpec(memory_space=pltpu.SMEM)
    n_cut = 4
    scratch = [
        v((2, rows, feat_half), bf), v((2, heads, 128), f32), v((rows, feats), bf),
        v(wqs.shape, bf), v(wks.shape, bf), v(wvs.shape, bf), v(wqw.shape, bf), v(wkw.shape, bf),
        v(wvw.shape, bf), v(wos.shape, bf), v(wow.shape, bf),
        v((heads, 2, half, wide), bf), v((heads, 2, half // 2, wide), bf),
        v((n_sp, 2, half, wide), bf), v((n_sp, half // 2, wide), bf),
        v((n_sp * half, wide), bf), v((4 * half, n_sp * rows), f32),
        v((rows, kvw_cols), bf), v((rows, kvw_cols), bf), v((rows, sw), bf),
        v((n_sp, half // 2, wide), bf), v((heads, 2, half // 2, wide), bf), v((rows, sw), f32),
        v((2, rows, 128), f32), v((2, rows, 128), f32), v((rows, feats), f32), v((rows, feats), f32),
        v((n_cut, half, feats // n_cut), bf), v((n_cut, half, feats // n_cut), bf),
        dma((8,)), dma, dma, dma, dma, dma, dma((heads, 2)), dma((n_sp,)), dma((heads, 2)), dma((n_sp,)),
        dma((n_sp,)), dma((n_sp,)), dma, dma, dma((n_sp,)), dma((heads, 2)), dma((2,)), dma((2,)),
        dma((n_cut,)), dma((n_cut,)),
    ]
    return pl.pallas_call(
        functools.partial(kernel, n_sp),
        out_shape=jax.ShapeDtypeStruct((half, feats), bf),
        in_specs=[anywhere, vmem] + [anywhere] * 6 + [smem, smem, vmem, vmem, anywhere, anywhere, vmem],
        out_specs=vmem,
        scratch_shapes=scratch,
        compiler_params=pltpu.CompilerParams(
            collective_id=0, has_side_effects=True, vmem_limit_bytes=48 * 1024 * 1024
        ),
        name="layer",
    )(*args)


def passed_along(value, axis, steps):
    count = lax.axis_size(axis)
    initial, last = (max(0, -steps), min(count, count - steps))
    return lax.ppermute(value, axis, [(source, source + steps) for source in range(initial, last)])


def rounded(values):
    return lax.optimization_barrier(values.astype(jnp.bfloat16)).astype(jnp.float32)


def norm_rows(values, gain):
    stats = jnp.mean(values * values, axis=-1, keepdims=True)
    return values * lax.rsqrt(stats + EPS) * gain


def stick_block(queries, key_pair, head_bias, key_mask, carried):
    result, logsum = carried
    head_count = queries.shape[1]
    key_rows = key_pair[0].reshape(key_pair.shape[1], head_count, HEAD_DIM)
    values = key_pair[1].reshape(key_pair.shape[1], head_count, HEAD_DIM)
    scores = jnp.einsum(
        "thd,shd->hts", queries, key_rows, preferred_element_type=jnp.float32
    ) * HEAD_DIM ** (-0.5)
    scores = scores + head_bias[:, None, None]
    usable = key_mask[None]
    log_keep = jnp.where(usable, jax.nn.log_sigmoid(-scores), 0.0)
    suffix = lax.cumsum(log_keep, axis=2, reverse=True) - log_keep
    stick_weights = jnp.where(
        usable, jnp.exp(jax.nn.log_sigmoid(scores) + suffix + logsum[:, :, None]), 0.0
    )
    stick_weights = stick_weights.astype(jnp.bfloat16)
    result = result + jnp.einsum(
        "hts,shd->htd", stick_weights, values, preferred_element_type=jnp.float32
    )
    logsum = logsum + jnp.sum(log_keep, axis=2)
    return (result, logsum)


def by_collectives(
    tokens,
    pre_gain,
    w_query_stick,
    w_key_stick,
    w_value_stick,
    w_query_window,
    w_key_window,
    w_value_window,
    stick_bias,
    sinks,
    stick_gain,
    window_gain,
    w_out_stick,
    w_out_window,
    post_gain,
):
    gathered = lax.all_gather(tokens, "tp", axis=1, tiled=True)
    normed = norm_rows(gathered.astype(jnp.float32), pre_gain).astype(jnp.bfloat16)

    def project(weight):
        return jnp.dot(normed, weight, preferred_element_type=jnp.float32).astype(jnp.bfloat16)

    tok_rows = normed.shape[0]
    dev_index = lax.axis_index("sp")
    dev_count = lax.axis_size("sp")
    query_stick = project(w_query_stick)
    stick_heads = query_stick.shape[1] // HEAD_DIM
    queries = query_stick.reshape(tok_rows, stick_heads, HEAD_DIM)
    own_pair = jnp.stack([project(w_key_stick), project(w_value_stick)])
    pair_width = own_pair.shape[2]
    positions = jnp.arange(tok_rows, dtype=jnp.int32)
    initial = (
        jnp.zeros((stick_heads, tok_rows, HEAD_DIM), jnp.float32),
        jnp.zeros((stick_heads, tok_rows), jnp.float32),
    )
    collected = own_pair[None]
    for section_index in range(dev_count.bit_length() - 1):
        arrived = passed_along(collected, "sp", 2**section_index)
        collected = jnp.concatenate([arrived, collected], axis=0)
    per_group = min(dev_count, 8)
    group_count = dev_count // per_group
    grouped = collected.reshape(group_count, per_group, 2, tok_rows, pair_width)
    grouped = grouped.transpose(0, 2, 1, 3, 4).reshape(
        group_count, 2, per_group * tok_rows, pair_width
    )
    first_source = dev_index - (dev_count - 1)
    group_starts = (first_source + jnp.arange(group_count, dtype=jnp.int32) * per_group) * tok_rows
    query_pos = dev_index * tok_rows + positions
    span_offs = jnp.arange(per_group * tok_rows, dtype=jnp.int32)

    def visit_group(carried, inputs):
        key_pair, start_pos = inputs
        key_pos = start_pos + span_offs
        key_mask = (key_pos[None, :] >= 0) & (key_pos[None, :] < query_pos[:, None])
        return (stick_block(queries, key_pair, stick_bias, key_mask, carried), None)

    (stick_sum, _), _ = lax.scan(visit_group, initial, (grouped, group_starts), reverse=True)
    stick_out = (
        stick_sum.transpose(1, 0, 2).reshape(tok_rows, stick_heads * HEAD_DIM).astype(jnp.bfloat16)
    )
    query_window = project(w_query_window)
    window_pair = jnp.stack([project(w_key_window), project(w_value_window)])
    kv_heads = window_pair.shape[2] // HEAD_DIM
    previous = passed_along(window_pair, "sp", 1)
    extended = jnp.concatenate([previous, window_pair], axis=1)
    block_count = tok_rows // WINDOW
    extended = extended.reshape(2, block_count + 1, WINDOW, kv_heads, HEAD_DIM)
    banded = jnp.concatenate([extended[:, :-1], extended[:, 1:]], axis=2)
    q_blocks = query_window.reshape(block_count, WINDOW, kv_heads, GROUP, HEAD_DIM)
    logits = jnp.einsum(
        "nqhgd,nchd->nhgqc", q_blocks, banded[0], preferred_element_type=jnp.float32
    ) * HEAD_DIM ** (-0.5)
    query_offs = jnp.arange(WINDOW, dtype=jnp.int32)[:, None]
    key_offs = jnp.arange(2 * WINDOW, dtype=jnp.int32)[None, :]
    distance = query_offs + WINDOW - key_offs
    key_pos = (
        dev_index * tok_rows
        + jnp.arange(block_count, dtype=jnp.int32)[:, None] * WINDOW
        - WINDOW
        + key_offs
    )
    usable = ((distance >= 0) & (distance < WINDOW))[None] & (key_pos >= 0)[:, None, :]
    logits = jnp.where(usable[:, None, None], logits, -jnp.inf)
    sink_logit = sinks.reshape(kv_heads, GROUP)[None, :, :, None, None]
    row_top = jnp.maximum(jnp.max(logits, axis=-1, keepdims=True), sink_logit)
    weights_exp = jnp.exp(logits - row_top)
    normalizer = jnp.sum(weights_exp, axis=-1, keepdims=True) + jnp.exp(sink_logit - row_top)
    window_weights = (weights_exp / normalizer).astype(jnp.bfloat16)
    window_sum = jnp.einsum(
        "nhgqc,nchd->nqhgd", window_weights, banded[1], preferred_element_type=jnp.float32
    )
    window_out = window_sum.reshape(tok_rows, query_window.shape[1]).astype(jnp.bfloat16)
    stick_float = stick_out.astype(jnp.float32)
    window_float = window_out.astype(jnp.float32)
    squares = lax.psum(
        (jnp.sum(stick_float * stick_float, axis=1), jnp.sum(window_float * window_float, axis=1)),
        "tp",
    )
    stick_normed = (
        stick_float * lax.rsqrt(squares[0][:, None] / (stick_gain.shape[0] * lax.axis_size("tp")) + EPS) * stick_gain
    ).astype(jnp.bfloat16)
    window_normed = (
        window_float * lax.rsqrt(squares[1][:, None] / (window_gain.shape[0] * lax.axis_size("tp")) + EPS) * window_gain
    ).astype(jnp.bfloat16)
    total = jnp.dot(stick_normed, w_out_stick, preferred_element_type=jnp.float32)
    combined = lax.psum_scatter(
        (total + jnp.dot(window_normed, w_out_window, preferred_element_type=jnp.float32)).astype(
            jnp.bfloat16
        ),
        "tp",
        scatter_dimension=0,
        tiled=True,
    ).astype(jnp.float32)
    combined = rounded(combined)
    return norm_rows(combined, post_gain).astype(jnp.bfloat16)


def solution(mesh):
    in_specs = (
        P("sp", "tp"),
        P(),
        P(None, "tp"),
        P(None, "tp"),
        P(None, "tp"),
        P(None, "tp"),
        P(None, "tp"),
        P(None, "tp"),
        P("tp"),
        P("tp"),
        P("tp"),
        P("tp"),
        P("tp", None),
        P("tp", None),
        P(),
    )
    n_sp, n_tp = mesh.shape["sp"], mesh.shape["tp"]

    def shards(*args):
        heads = args[2].shape[1] // HEAD_DIM
        if n_tp == 2 and n_tp * heads == n_sp and args[0].shape[0] == WINDOW and n_sp % 4 == 0:
            return one_kernel(n_sp, *args)
        return by_collectives(*args)

    return jax.shard_map(
        shards,
        mesh=mesh,
        in_specs=in_specs,
        out_specs=P(("sp", "tp"), None),
        check_vma=False,
    )
```

```python
import functools

import jax
import jax.numpy as jnp
from jax import lax
from jax.experimental import pallas as pl
from jax.experimental.pallas import tpu as pltpu
from jax.sharding import PartitionSpec as P

HEAD_DIM = 64
GROUP = 2
WINDOW = 128
EPS = 1e-06
LOG2E = 1.4426950408889634
MESH = pl.DeviceIdType.MESH


def dot(a, b):
    return jnp.dot(a, b, preferred_element_type=jnp.float32)


def dot_t(a, b):
    return lax.dot_general(a, b, (((1,), (1,)), ((), ())), preferred_element_type=jnp.float32)


def kernel(
    n_sp,
    tokens, pre_gain_in, wqs, wks, wvs, wqw, wkw, wvw, bias_in, sinks_in, sgain_in, wgain_in, wos, wow,
    post_gain_in, out,
    pre_gain, bias, sinks, sgain, wgain, post_gain, x, bias_buf, normed, vqs, vks, vvs, vqw, vkw, vvw, vos, vow,
    kv_send, q_send, kv_all, q_all, q_pad, staged,
    kvw, kvw_prev, w_out_buf, o_send, o_recv, s_out_buf,
    sq_send, sq_recv, total_w, comb, c_send, c_recv,
    w_sem, tok_sem, x_ss, x_rs, b_ss, b_rs, kv_ss, kv_rs, q_ss, q_rs, f_ss, f_rs,
    p_ss, p_rs, o_ss, o_rs, sq_ss, sq_rs, c_ss, c_rs,
):
    bf = jnp.bfloat16
    f32 = jnp.float32
    s = lax.axis_index("sp")
    t = lax.axis_index("tp")
    other = 1 - t
    rows, feat_half = tokens.shape
    feats = 2 * feat_half
    half = rows // 2
    quarter = half // 2
    hd = HEAD_DIM
    heads = wqs.shape[1] // hd
    kv_heads = wkw.shape[1] // hd
    sw = wqs.shape[1]

    loads = [
        pltpu.make_async_copy(src, dst, w_sem.at[n])
        for n, (src, dst) in enumerate(
            [(wks, vks), (wvs, vvs), (wqs, vqs), (wkw, vkw), (wvw, vvw), (wqw, vqw), (wow, vow), (wos, vos),
             (bias_in, bias), (pre_gain_in, pre_gain), (sinks_in, sinks), (sgain_in, sgain),
             (wgain_in, wgain), (post_gain_in, post_gain)]
        )
    ]
    l_ks, l_vs, l_qs, l_kw, l_vw, l_qw, l_ow, l_os, l_bias, *l_small = loads
    tok_load = pltpu.make_async_copy(tokens, x.at[t], tok_sem)
    l_bias.start()
    tok_load.start()
    for load in l_small + loads[:8]:
        load.start()

    row_id = lax.broadcasted_iota(jnp.int32, (heads, 128), 0)
    bias_rows = jnp.zeros((heads, 128), f32)
    l_bias.wait()
    for i in range(heads):
        bias_rows = jnp.where(row_id == i, bias[i] * LOG2E, bias_rows)
    bias_buf[t] = bias_rows

    barrier = pltpu.get_barrier_semaphore()
    me = s * 2 + t

    def greet(k, carry):
        peer = lax.rem(me + k, 2 * n_sp)
        pl.semaphore_signal(
            barrier, inc=1, device_id={"sp": peer // 2, "tp": lax.rem(peer, 2)}, device_id_type=MESH
        )
        return carry

    lax.fori_loop(1, 2 * n_sp, greet, 0)
    for load in l_small:
        load.wait()
    tok_load.wait()
    pl.semaphore_wait(barrier, 2 * n_sp - 1)

    def to_partner(src, dst, ss, rs):
        return pltpu.make_async_remote_copy(
            src_ref=src, dst_ref=dst, send_sem=ss, recv_sem=rs,
            device_id={"sp": s, "tp": other}, device_id_type=MESH,
        )

    x_copy = to_partner(x.at[t], x.at[t], x_ss, x_rs)
    b_copy = to_partner(bias_buf.at[t], bias_buf.at[t], b_ss, b_rs)
    x_copy.start()
    b_copy.start()
    x_copy.wait_recv()

    gain = pre_gain[...].reshape(1, feats)

    def norm_step(n, carry):
        part = pl.ds(pl.multiple_of(n * 32, 32), 32)
        left = x[0, part, :].astype(f32)
        right = x[1, part, :].astype(f32)
        stats = (
            jnp.sum(left * left, axis=1, keepdims=True) + jnp.sum(right * right, axis=1, keepdims=True)
        ) * (1.0 / feats)
        inv = lax.rsqrt(stats + EPS)
        normed[part, :feat_half] = (left * inv * gain[:, :feat_half]).astype(bf)
        normed[part, feat_half:] = (right * inv * gain[:, feat_half:]).astype(bf)
        return carry

    lax.fori_loop(0, rows // 32, norm_step, 0)

    l_ks.wait()
    keys = dot(normed[...], vks[...])
    l_vs.wait()
    values = dot(normed[...], vvs[...])
    for i in range(heads):
        cols = slice(i * hd, (i + 1) * hd)
        packed = jnp.concatenate([keys[:, cols], values[:, cols]], axis=1).astype(bf)
        kv_send[i] = packed.reshape(2, half, 2 * hd)

    def scatter(send, slots, ss, rs):
        def step(k, carry):
            i = lax.rem(k // 2 + s, heads)
            u = lax.rem(k, 2)
            chip = t * heads + i
            is_self = jnp.logical_and(chip == s, u == t)

            @pl.when(is_self)
            def _():
                pltpu.make_async_copy(send.at[i, u], slots(u), rs.at[s]).start()

            @pl.when(jnp.logical_not(is_self))
            def _():
                pltpu.make_async_remote_copy(
                    src_ref=send.at[i, u], dst_ref=slots(u), send_sem=ss.at[i, u], recv_sem=rs.at[s],
                    device_id={"sp": chip, "tp": u}, device_id_type=MESH,
                ).start()

            return carry

        lax.fori_loop(0, 2 * heads, step, 0)

    def scatter_done(send, slots, ss, rs):
        def step(k, carry):
            i = k // 2
            u = lax.rem(k, 2)
            chip = t * heads + i
            is_self = jnp.logical_and(chip == s, u == t)

            @pl.when(jnp.logical_not(is_self))
            def _():
                pltpu.make_async_remote_copy(
                    src_ref=send.at[i, u], dst_ref=slots(u), send_sem=ss.at[i, u], recv_sem=rs.at[s],
                    device_id={"sp": chip, "tp": u}, device_id_type=MESH,
                ).wait_send()

            return carry

        lax.fori_loop(0, 2 * heads, step, 0)

    kv_slot = lambda u: kv_all.at[s, u]
    q_slot = lambda u: q_all.at[s]
    scatter(kv_send, kv_slot, kv_ss, kv_rs)

    l_qs.wait()
    queries = dot(normed[...], vqs[...])
    for i in range(heads):
        cols = slice(i * hd, (i + 1) * hd)
        for u in range(2):
            top = queries[u * half : u * half + quarter, cols]
            low = queries[u * half + quarter : (u + 1) * half, cols]
            q_send[i, u] = jnp.concatenate([top, low], axis=1).astype(bf)
    scatter(q_send, q_slot, q_ss, q_rs)

    l_kw.wait()
    kvw[:, : kv_heads * hd] = dot(normed[...], vkw[...]).astype(bf)
    l_vw.wait()
    kvw[:, kv_heads * hd :] = dot(normed[...], vvw[...]).astype(bf)
    prev_copy = lambda to: pltpu.make_async_remote_copy(
        src_ref=kvw, dst_ref=kvw_prev, send_sem=p_ss, recv_sem=p_rs,
        device_id={"sp": to, "tp": t}, device_id_type=MESH,
    )

    @pl.when(s < n_sp - 1)
    def _():
        prev_copy(s + 1).start()

    l_qw.wait()
    qw = dot(normed[...], vqw[...])

    @pl.when(s == 0)
    def _():
        kvw_prev[...] = jnp.zeros_like(kvw_prev)

    @pl.when(s > 0)
    def _():
        prev_copy(s - 1).wait_recv()

    def forward(k, carry):
        src = n_sp - 1 - k
        pltpu.make_async_remote_copy(
            src_ref=kv_send.at[0, 0], dst_ref=kv_all.at[src, t], send_sem=kv_ss.at[0, 0],
            recv_sem=kv_rs.at[src], device_id={"sp": s, "tp": other}, device_id_type=MESH,
        ).wait_recv()
        to_partner(kv_all.at[src, t], kv_all.at[src, t], f_ss.at[src], f_rs.at[src]).start()
        return carry

    def forward_arrived(k, carry):
        to_partner(kv_all.at[k, other], kv_all.at[k, other], f_ss.at[k], f_rs.at[k]).wait_recv()
        return carry

    def forward_sent(k, carry):
        to_partner(kv_all.at[k, t], kv_all.at[k, t], f_ss.at[k], f_rs.at[k]).wait_send()
        return carry

    two = 2 * rows
    r_iota = lax.broadcasted_iota(jnp.int32, (two, two), 0)
    c_iota = lax.broadcasted_iota(jnp.int32, (two, two), 1)
    dist = lax.rem(r_iota, rows) + rows - c_iota
    in_window = (dist >= 0) & (dist < WINDOW) & ((c_iota >= rows) | (s > 0))
    first_rows = lax.broadcasted_iota(jnp.int32, (two, 1), 0) < rows
    for g in range(kv_heads):
        cols = slice(g * hd, (g + 1) * hd)
        v_cols = slice((kv_heads + g) * hd, (kv_heads + g + 1) * hd)
        kk = jnp.concatenate([kvw_prev[:, cols], kvw[:, cols]], axis=0)
        vv = jnp.concatenate([kvw_prev[:, v_cols], kvw[:, v_cols]], axis=0)
        base = g * GROUP * hd
        qq = jnp.concatenate(
            [qw[:, base : base + hd], qw[:, base + hd : base + 2 * hd]], axis=0
        ).astype(bf)
        logits = jnp.where(in_window, dot_t(qq, kk) * hd**-0.5, -jnp.inf)
        sink = jnp.where(first_rows, sinks[GROUP * g], sinks[GROUP * g + 1])
        top = jnp.maximum(jnp.max(logits, axis=1, keepdims=True), sink)
        grown = jnp.exp(logits - top)
        total = jnp.sum(grown, axis=1, keepdims=True) + jnp.exp(sink - top)
        weights = (grown / total).astype(bf)
        res = dot(weights, vv)
        w_out_buf[:, base : base + 2 * hd] = jnp.concatenate([res[:rows], res[rows:]], axis=1).astype(bf)

    wf = w_out_buf[...].astype(f32)
    sq_send[0] = jnp.broadcast_to(jnp.sum(wf * wf, axis=1, keepdims=True), (rows, 128))

    lax.fori_loop(0, n_sp, forward, 0)
    sq_w = to_partner(sq_send.at[0], sq_recv.at[0], sq_ss.at[0], sq_rs.at[0])
    sq_w.start()

    def take_q(k, carry):
        pltpu.make_async_remote_copy(
            src_ref=q_send.at[0, 0], dst_ref=q_all.at[k], send_sem=q_ss.at[0, 0],
            recv_sem=q_rs.at[k], device_id={"sp": s, "tp": other}, device_id_type=MESH,
        ).wait_recv()
        slab = q_all[k].astype(f32)
        zero = jnp.zeros((quarter, hd), f32)
        both = jnp.concatenate(
            [
                jnp.concatenate([slab[:, :hd], zero], axis=1),
                jnp.concatenate([slab[:, hd:], zero], axis=1),
            ],
            axis=0,
        )
        q_pad[pl.ds(pl.multiple_of(k * half, half), half), :] = both.astype(bf)
        return carry

    lax.fori_loop(0, n_sp, take_q, 0)
    lax.fori_loop(0, n_sp, forward_arrived, 0)
    b_copy.wait_recv()
    head_bias = bias_buf[s // heads, pl.ds(lax.rem(s, heads), 1), :][:, :1]

    kt = 2 * rows
    chunk = 4 * half
    later = (
        lax.broadcasted_iota(jnp.int32, (kt, kt), 0) > lax.broadcasted_iota(jnp.int32, (kt, kt), 1)
    ).astype(bf)
    row = lax.broadcasted_iota(jnp.int32, (chunk, kt), 0)
    lane = lax.broadcasted_iota(jnp.int32, (chunk, kt), 1)
    q_at = (row // half) * rows + t * half + lax.rem(row, half)
    scale = LOG2E * hd**-0.5

    def tile_of(n):
        return kv_all[2 * n : 2 * n + 2].reshape(kt, 2 * hd)

    owner = s // heads
    slot = lax.rem(s, heads)
    for qc in reversed(range(n_sp // 4)):
        last = 2 * qc + 1
        carry = jnp.zeros((chunk, 1), f32)
        carries = {}
        for n in range(last, -1, -1):
            low = chunk // 2 if n == last else 0
            qs = q_pad[qc * chunk + low : (qc + 1) * chunk, :]
            z = dot_t(qs, tile_of(n)) * scale + head_bias
            pos = jnp.maximum(z, 0.0)
            neg = z - pos
            soft = jnp.log2(1.0 + jnp.exp2(neg - pos))
            drop = pos + soft
            hold = neg - soft
            if n >= last - 1:
                usable = (lane + (n - 2 * qc) * kt < q_at)[low:]
                drop = jnp.where(usable, drop, 0.0)
                hold = jnp.where(usable, hold, -jnp.inf)
            suffix = dot(drop.astype(bf), later)
            staged[low:, n * kt : (n + 1) * kt] = hold - suffix
            carries[n] = carry[low:]
            step = suffix[:, :1] + drop[:, :1]
            if low:
                step = jnp.concatenate([jnp.zeros((low, 1), f32), step], axis=0)
            carry = carry + step
        acc = None
        for n in range(last - 1, -1, -1):
            weights = jnp.exp2(staged[:, n * kt : (n + 1) * kt] - carries[n]).astype(bf)
            res = dot(weights, tile_of(n))
            acc = res if acc is None else acc + res
        low = chunk // 2
        weights = jnp.exp2(staged[low:, last * kt : (last + 1) * kt] - carries[last]).astype(bf)
        tail = dot(weights, tile_of(last))
        acc = jnp.concatenate([acc[:low], acc[low:] + tail], axis=0)
        for b in range(4):
            top = acc[b * half : b * half + quarter, hd:]
            bot = acc[b * half + quarter : (b + 1) * half, hd:]
            o_send[qc * 4 + b] = jnp.concatenate([top, bot], axis=1).astype(bf)

        def give(k, carry):
            is_self = jnp.logical_and(k == s, t == owner)

            @pl.when(is_self)
            def _():
                pltpu.make_async_copy(o_send.at[k], o_recv.at[slot, t], o_rs.at[slot, t]).start()

            @pl.when(jnp.logical_not(is_self))
            def _():
                pltpu.make_async_remote_copy(
                    src_ref=o_send.at[k], dst_ref=o_recv.at[slot, t], send_sem=o_ss.at[k],
                    recv_sem=o_rs.at[slot, t], device_id={"sp": k, "tp": owner}, device_id_type=MESH,
                ).start()

            return carry

        lax.fori_loop(qc * 4, qc * 4 + 4, give, 0)

    l_ow.wait()
    total_w[...] = dot((wf * wgain[...].reshape(1, sw)).astype(bf), vow[...])
    sq_w.wait_recv()
    sw_cols = 2.0 * sw
    inv_w = lax.rsqrt((sq_send[0] + sq_recv[0])[:, :1] / sw_cols + EPS)

    def take_o(k, carry):
        pltpu.make_async_remote_copy(
            src_ref=o_send.at[0], dst_ref=o_recv.at[k // 2, lax.rem(k, 2)], send_sem=o_ss.at[0],
            recv_sem=o_rs.at[k // 2, lax.rem(k, 2)], device_id={"sp": s, "tp": other}, device_id_type=MESH,
        ).wait_recv()
        return carry

    lax.fori_loop(0, 2 * heads, take_o, 0)
    for j in range(heads // 2):
        for u in range(2):
            one = o_recv[2 * j, u].astype(f32)
            two_ = o_recv[2 * j + 1, u].astype(f32)
            s_out_buf[u * half : u * half + quarter, 2 * j * hd : 2 * (j + 1) * hd] = jnp.concatenate(
                [one[:, :hd], two_[:, :hd]], axis=1
            )
            s_out_buf[u * half + quarter : (u + 1) * half, 2 * j * hd : 2 * (j + 1) * hd] = jnp.concatenate(
                [one[:, hd:], two_[:, hd:]], axis=1
            )
    sf = s_out_buf[...]
    sq_send[1] = jnp.broadcast_to(jnp.sum(sf * sf, axis=1, keepdims=True), (rows, 128))
    gained = (sf * sgain[...].reshape(1, sw)).astype(bf)
    sq_s = to_partner(sq_send.at[1], sq_recv.at[1], sq_ss.at[1], sq_rs.at[1])
    sq_s.start()
    l_os.wait()
    n_cut = c_send.shape[0]
    cut = feats // n_cut
    for n in range(n_cut):
        comb[:, n * cut : (n + 1) * cut] = dot(gained, vos[:, n * cut : (n + 1) * cut])
    sq_s.wait_recv()
    inv_s = lax.rsqrt((sq_send[1] + sq_recv[1])[:, :1] / sw_cols + EPS)
    copies = []
    theirs = pl.ds(pl.multiple_of(other * half, half), half)
    mine = pl.ds(pl.multiple_of(t * half, half), half)
    for n in range(n_cut):
        cols = slice(n * cut, (n + 1) * cut)
        comb[:, cols] = comb[:, cols] * inv_s + total_w[:, cols] * inv_w
        c_send[n] = comb[theirs, cols].astype(bf)
        copy = to_partner(c_send.at[n], c_recv.at[n], c_ss.at[n], c_rs.at[n])
        copy.start()
        copies.append(copy)
    square = jnp.zeros((half, 1), f32)
    for n in range(n_cut):
        cols = slice(n * cut, (n + 1) * cut)
        copies[n].wait_recv()
        summed = (comb[mine, cols] + c_recv[n].astype(f32)).astype(bf).astype(f32)
        total_w[:half, cols] = summed
        square = square + jnp.sum(summed * summed, axis=1, keepdims=True)
    inv = lax.rsqrt(square / feats + EPS)
    out[...] = (total_w[:half, :] * inv * post_gain[...].reshape(1, feats)).astype(bf)

    x_copy.wait_send()
    b_copy.wait_send()
    scatter_done(kv_send, kv_slot, kv_ss, kv_rs)
    scatter_done(q_send, q_slot, q_ss, q_rs)
    lax.fori_loop(0, n_sp, forward_sent, 0)

    @pl.when(s < n_sp - 1)
    def _():
        prev_copy(s + 1).wait_send()

    def gave(k, carry):
        @pl.when(jnp.logical_not(jnp.logical_and(k == s, t == owner)))
        def _():
            pltpu.make_async_remote_copy(
                src_ref=o_send.at[k], dst_ref=o_recv.at[slot, t], send_sem=o_ss.at[k],
                recv_sem=o_rs.at[slot, t], device_id={"sp": k, "tp": owner}, device_id_type=MESH,
            ).wait_send()

        return carry

    lax.fori_loop(0, n_sp, gave, 0)
    sq_w.wait_send()
    sq_s.wait_send()
    for copy in copies:
        copy.wait_send()


def one_kernel(n_sp, *args):
    tokens, pre_gain, wqs, wks, wvs, wqw, wkw, wvw, bias, sinks, sgain, wgain, wos, wow, post_gain = args
    bf = jnp.bfloat16
    f32 = jnp.float32
    rows, feat_half = tokens.shape
    feats = 2 * feat_half
    half = rows // 2
    hd = HEAD_DIM
    heads = wqs.shape[1] // hd
    sw = wqs.shape[1]
    wide = 2 * hd
    kvw_cols = wkw.shape[1] + wvw.shape[1]
    assert 2 * heads == n_sp and rows == WINDOW
    v = pltpu.VMEM
    dma = pltpu.SemaphoreType.DMA
    anywhere = pl.BlockSpec(memory_space=pl.ANY)
    vmem = pl.BlockSpec(memory_space=pltpu.VMEM)
    n_cut = 4
    scratch = [
        v(pre_gain.shape, f32), pltpu.SMEM(bias.shape, f32), pltpu.SMEM(sinks.shape, f32),
        v(sgain.shape, f32), v(wgain.shape, f32), v(post_gain.shape, f32),
        v((2, rows, feat_half), bf), v((2, heads, 128), f32), v((rows, feats), bf),
        v(wqs.shape, bf), v(wks.shape, bf), v(wvs.shape, bf), v(wqw.shape, bf), v(wkw.shape, bf),
        v(wvw.shape, bf), v(wos.shape, bf), v(wow.shape, bf),
        v((heads, 2, half, wide), bf), v((heads, 2, half // 2, wide), bf),
        v((n_sp, 2, half, wide), bf), v((n_sp, half // 2, wide), bf),
        v((n_sp * half, wide), bf), v((4 * half, n_sp * rows), f32),
        v((rows, kvw_cols), bf), v((rows, kvw_cols), bf), v((rows, sw), bf),
        v((n_sp, half // 2, wide), bf), v((heads, 2, half // 2, wide), bf), v((rows, sw), f32),
        v((2, rows, 128), f32), v((2, rows, 128), f32), v((rows, feats), f32), v((rows, feats), f32),
        v((n_cut, half, feats // n_cut), bf), v((n_cut, half, feats // n_cut), bf),
        dma((14,)), dma, dma, dma, dma, dma, dma((heads, 2)), dma((n_sp,)), dma((heads, 2)), dma((n_sp,)),
        dma((n_sp,)), dma((n_sp,)), dma, dma, dma((n_sp,)), dma((heads, 2)), dma((2,)), dma((2,)),
        dma((n_cut,)), dma((n_cut,)),
    ]
    return pl.pallas_call(
        functools.partial(kernel, n_sp),
        out_shape=jax.ShapeDtypeStruct((half, feats), bf),
        in_specs=[anywhere] * len(args),
        out_specs=vmem,
        scratch_shapes=scratch,
        compiler_params=pltpu.CompilerParams(
            collective_id=0, has_side_effects=True, vmem_limit_bytes=67043328
        ),
        name="layer",
    )(*args)


def passed_along(value, axis, steps):
    count = lax.axis_size(axis)
    initial, last = (max(0, -steps), min(count, count - steps))
    return lax.ppermute(value, axis, [(source, source + steps) for source in range(initial, last)])


def rounded(values):
    return lax.optimization_barrier(values.astype(jnp.bfloat16)).astype(jnp.float32)


def norm_rows(values, gain):
    stats = jnp.mean(values * values, axis=-1, keepdims=True)
    return values * lax.rsqrt(stats + EPS) * gain


def stick_block(queries, key_pair, head_bias, key_mask, carried):
    result, logsum = carried
    head_count = queries.shape[1]
    key_rows = key_pair[0].reshape(key_pair.shape[1], head_count, HEAD_DIM)
    values = key_pair[1].reshape(key_pair.shape[1], head_count, HEAD_DIM)
    scores = jnp.einsum(
        "thd,shd->hts", queries, key_rows, preferred_element_type=jnp.float32
    ) * HEAD_DIM ** (-0.5)
    scores = scores + head_bias[:, None, None]
    usable = key_mask[None]
    log_keep = jnp.where(usable, jax.nn.log_sigmoid(-scores), 0.0)
    suffix = lax.cumsum(log_keep, axis=2, reverse=True) - log_keep
    stick_weights = jnp.where(
        usable, jnp.exp(jax.nn.log_sigmoid(scores) + suffix + logsum[:, :, None]), 0.0
    )
    stick_weights = stick_weights.astype(jnp.bfloat16)
    result = result + jnp.einsum(
        "hts,shd->htd", stick_weights, values, preferred_element_type=jnp.float32
    )
    logsum = logsum + jnp.sum(log_keep, axis=2)
    return (result, logsum)


def by_collectives(
    tokens,
    pre_gain,
    w_query_stick,
    w_key_stick,
    w_value_stick,
    w_query_window,
    w_key_window,
    w_value_window,
    stick_bias,
    sinks,
    stick_gain,
    window_gain,
    w_out_stick,
    w_out_window,
    post_gain,
):
    gathered = lax.all_gather(tokens, "tp", axis=1, tiled=True)
    normed = norm_rows(gathered.astype(jnp.float32), pre_gain).astype(jnp.bfloat16)

    def project(weight):
        return jnp.dot(normed, weight, preferred_element_type=jnp.float32).astype(jnp.bfloat16)

    tok_rows = normed.shape[0]
    dev_index = lax.axis_index("sp")
    dev_count = lax.axis_size("sp")
    query_stick = project(w_query_stick)
    stick_heads = query_stick.shape[1] // HEAD_DIM
    queries = query_stick.reshape(tok_rows, stick_heads, HEAD_DIM)
    own_pair = jnp.stack([project(w_key_stick), project(w_value_stick)])
    pair_width = own_pair.shape[2]
    positions = jnp.arange(tok_rows, dtype=jnp.int32)
    initial = (
        jnp.zeros((stick_heads, tok_rows, HEAD_DIM), jnp.float32),
        jnp.zeros((stick_heads, tok_rows), jnp.float32),
    )
    collected = own_pair[None]
    for section_index in range(dev_count.bit_length() - 1):
        arrived = passed_along(collected, "sp", 2**section_index)
        collected = jnp.concatenate([arrived, collected], axis=0)
    per_group = min(dev_count, 8)
    group_count = dev_count // per_group
    grouped = collected.reshape(group_count, per_group, 2, tok_rows, pair_width)
    grouped = grouped.transpose(0, 2, 1, 3, 4).reshape(
        group_count, 2, per_group * tok_rows, pair_width
    )
    first_source = dev_index - (dev_count - 1)
    group_starts = (first_source + jnp.arange(group_count, dtype=jnp.int32) * per_group) * tok_rows
    query_pos = dev_index * tok_rows + positions
    span_offs = jnp.arange(per_group * tok_rows, dtype=jnp.int32)

    def visit_group(carried, inputs):
        key_pair, start_pos = inputs
        key_pos = start_pos + span_offs
        key_mask = (key_pos[None, :] >= 0) & (key_pos[None, :] < query_pos[:, None])
        return (stick_block(queries, key_pair, stick_bias, key_mask, carried), None)

    (stick_sum, _), _ = lax.scan(visit_group, initial, (grouped, group_starts), reverse=True)
    stick_out = (
        stick_sum.transpose(1, 0, 2).reshape(tok_rows, stick_heads * HEAD_DIM).astype(jnp.bfloat16)
    )
    query_window = project(w_query_window)
    window_pair = jnp.stack([project(w_key_window), project(w_value_window)])
    kv_heads = window_pair.shape[2] // HEAD_DIM
    previous = passed_along(window_pair, "sp", 1)
    extended = jnp.concatenate([previous, window_pair], axis=1)
    block_count = tok_rows // WINDOW
    extended = extended.reshape(2, block_count + 1, WINDOW, kv_heads, HEAD_DIM)
    banded = jnp.concatenate([extended[:, :-1], extended[:, 1:]], axis=2)
    q_blocks = query_window.reshape(block_count, WINDOW, kv_heads, GROUP, HEAD_DIM)
    logits = jnp.einsum(
        "nqhgd,nchd->nhgqc", q_blocks, banded[0], preferred_element_type=jnp.float32
    ) * HEAD_DIM ** (-0.5)
    query_offs = jnp.arange(WINDOW, dtype=jnp.int32)[:, None]
    key_offs = jnp.arange(2 * WINDOW, dtype=jnp.int32)[None, :]
    distance = query_offs + WINDOW - key_offs
    key_pos = (
        dev_index * tok_rows
        + jnp.arange(block_count, dtype=jnp.int32)[:, None] * WINDOW
        - WINDOW
        + key_offs
    )
    usable = ((distance >= 0) & (distance < WINDOW))[None] & (key_pos >= 0)[:, None, :]
    logits = jnp.where(usable[:, None, None], logits, -jnp.inf)
    sink_logit = sinks.reshape(kv_heads, GROUP)[None, :, :, None, None]
    row_top = jnp.maximum(jnp.max(logits, axis=-1, keepdims=True), sink_logit)
    weights_exp = jnp.exp(logits - row_top)
    normalizer = jnp.sum(weights_exp, axis=-1, keepdims=True) + jnp.exp(sink_logit - row_top)
    window_weights = (weights_exp / normalizer).astype(jnp.bfloat16)
    window_sum = jnp.einsum(
        "nhgqc,nchd->nqhgd", window_weights, banded[1], preferred_element_type=jnp.float32
    )
    window_out = window_sum.reshape(tok_rows, query_window.shape[1]).astype(jnp.bfloat16)
    stick_float = stick_out.astype(jnp.float32)
    window_float = window_out.astype(jnp.float32)
    squares = lax.psum(
        (jnp.sum(stick_float * stick_float, axis=1), jnp.sum(window_float * window_float, axis=1)),
        "tp",
    )
    stick_normed = (
        stick_float * lax.rsqrt(squares[0][:, None] / (stick_gain.shape[0] * lax.axis_size("tp")) + EPS) * stick_gain
    ).astype(jnp.bfloat16)
    window_normed = (
        window_float * lax.rsqrt(squares[1][:, None] / (window_gain.shape[0] * lax.axis_size("tp")) + EPS) * window_gain
    ).astype(jnp.bfloat16)
    total = jnp.dot(stick_normed, w_out_stick, preferred_element_type=jnp.float32)
    combined = lax.psum_scatter(
        (total + jnp.dot(window_normed, w_out_window, preferred_element_type=jnp.float32)).astype(
            jnp.bfloat16
        ),
        "tp",
        scatter_dimension=0,
        tiled=True,
    ).astype(jnp.float32)
    combined = rounded(combined)
    return norm_rows(combined, post_gain).astype(jnp.bfloat16)


def solution(mesh):
    in_specs = (
        P("sp", "tp"),
        P(),
        P(None, "tp"),
        P(None, "tp"),
        P(None, "tp"),
        P(None, "tp"),
        P(None, "tp"),
        P(None, "tp"),
        P("tp"),
        P("tp"),
        P("tp"),
        P("tp"),
        P("tp", None),
        P("tp", None),
        P(),
    )
    n_sp, n_tp = mesh.shape["sp"], mesh.shape["tp"]

    def shards(*args):
        heads = args[2].shape[1] // HEAD_DIM
        if n_tp == 2 and n_tp * heads == n_sp and args[0].shape[0] == WINDOW and n_sp % 4 == 0:
            return one_kernel(n_sp, *args)
        return by_collectives(*args)

    return jax.shard_map(
        shards,
        mesh=mesh,
        in_specs=in_specs,
        out_specs=P(("sp", "tp"), None),
        check_vma=False,
    )
```

```python
import functools

import jax
import jax.numpy as jnp
from jax import lax
from jax.experimental import pallas as pl
from jax.experimental.pallas import tpu as pltpu
from jax.sharding import PartitionSpec as P

HEAD_DIM = 64
GROUP = 2
WINDOW = 128
EPS = 1e-06
LOG2E = 1.4426950408889634
MESH = pl.DeviceIdType.MESH


def dot(a, b):
    return jnp.dot(a, b, preferred_element_type=jnp.float32)


def dot_t(a, b):
    return lax.dot_general(a, b, (((1,), (1,)), ((), ())), preferred_element_type=jnp.float32)


def kernel(
    n_sp,
    tokens, pre_gain_in, wqs, wks, wvs, wqw, wkw, wvw, bias_in, sinks_in, sgain_in, wgain_in, wos, wow,
    post_gain_in, out,
    pre_gain, bias, sinks, sgain, wgain, post_gain, x, bias_buf, normed, vqs, vks, vvs, vqw, vkw, vvw, vos, vow,
    kv_send, q_send, kv_all, q_all, q_pad, staged,
    kvw, kvw_prev, w_out_buf, o_send, o_recv, s_out_buf,
    sq_send, sq_recv, total_w, comb, c_send, c_recv,
    w_sem, tok_sem, x_ss, x_rs, b_ss, b_rs, kv_ss, kv_rs, q_ss, q_rs, f_ss, f_rs,
    p_ss, p_rs, o_ss, o_rs, sq_ss, sq_rs, c_ss, c_rs,
):
    bf = jnp.bfloat16
    f32 = jnp.float32
    s = lax.axis_index("sp")
    t = lax.axis_index("tp")
    other = 1 - t
    rows, feat_half = tokens.shape
    feats = 2 * feat_half
    half = rows // 2
    quarter = half // 2
    hd = HEAD_DIM
    heads = wqs.shape[1] // hd
    kv_heads = wkw.shape[1] // hd
    sw = wqs.shape[1]

    barrier = pltpu.get_barrier_semaphore()
    me = s * 2 + t

    def greet(k, carry):
        peer = lax.rem(me + k, 2 * n_sp)
        pl.semaphore_signal(
            barrier, inc=1, device_id={"sp": peer // 2, "tp": lax.rem(peer, 2)}, device_id_type=MESH
        )
        return carry

    lax.fori_loop(1, 2 * n_sp, greet, 0)

    loads = [
        pltpu.make_async_copy(src, dst, w_sem.at[n])
        for n, (src, dst) in enumerate(
            [(wks, vks), (wvs, vvs), (wqs, vqs), (wkw, vkw), (wvw, vvw), (wqw, vqw), (wow, vow), (wos, vos),
             (bias_in, bias), (pre_gain_in, pre_gain), (sinks_in, sinks), (sgain_in, sgain),
             (wgain_in, wgain), (post_gain_in, post_gain)]
        )
    ]
    l_ks, l_vs, l_qs, l_kw, l_vw, l_qw, l_ow, l_os, l_bias, *l_small = loads
    tok_load = pltpu.make_async_copy(tokens, x.at[t], tok_sem)
    l_bias.start()
    tok_load.start()
    for load in l_small + loads[:8]:
        load.start()

    row_id = lax.broadcasted_iota(jnp.int32, (heads, 128), 0)
    bias_rows = jnp.zeros((heads, 128), f32)
    l_bias.wait()
    for i in range(heads):
        bias_rows = jnp.where(row_id == i, bias[i] * LOG2E, bias_rows)
    bias_buf[t] = bias_rows

    for load in l_small:
        load.wait()
    tok_load.wait()
    pl.semaphore_wait(barrier, 2 * n_sp - 1)

    def to_partner(src, dst, ss, rs):
        return pltpu.make_async_remote_copy(
            src_ref=src, dst_ref=dst, send_sem=ss, recv_sem=rs,
            device_id={"sp": s, "tp": other}, device_id_type=MESH,
        )

    x_copy = to_partner(x.at[t], x.at[t], x_ss, x_rs)
    b_copy = to_partner(bias_buf.at[t], bias_buf.at[t], b_ss, b_rs)
    x_copy.start()
    b_copy.start()
    x_copy.wait_recv()

    gain = pre_gain[...].reshape(1, feats)

    def norm_step(n, carry):
        part = pl.ds(pl.multiple_of(n * 32, 32), 32)
        left = x[0, part, :].astype(f32)
        right = x[1, part, :].astype(f32)
        stats = (
            jnp.sum(left * left, axis=1, keepdims=True) + jnp.sum(right * right, axis=1, keepdims=True)
        ) * (1.0 / feats)
        inv = lax.rsqrt(stats + EPS)
        normed[part, :feat_half] = (left * inv * gain[:, :feat_half]).astype(bf)
        normed[part, feat_half:] = (right * inv * gain[:, feat_half:]).astype(bf)
        return carry

    lax.fori_loop(0, rows // 32, norm_step, 0)

    l_ks.wait()
    keys = dot(normed[...], vks[...])
    l_vs.wait()
    values = dot(normed[...], vvs[...])
    for i in range(heads):
        cols = slice(i * hd, (i + 1) * hd)
        packed = jnp.concatenate([keys[:, cols], values[:, cols]], axis=1).astype(bf)
        kv_send[i] = packed.reshape(2, half, 2 * hd)

    def scatter(send, slots, ss, rs):
        def step(k, carry):
            i = lax.rem(k // 2 + s, heads)
            u = lax.rem(k, 2)
            chip = t * heads + i
            is_self = jnp.logical_and(chip == s, u == t)

            @pl.when(is_self)
            def _():
                pltpu.make_async_copy(send.at[i, u], slots(u), rs.at[s]).start()

            @pl.when(jnp.logical_not(is_self))
            def _():
                pltpu.make_async_remote_copy(
                    src_ref=send.at[i, u], dst_ref=slots(u), send_sem=ss.at[i, u], recv_sem=rs.at[s],
                    device_id={"sp": chip, "tp": u}, device_id_type=MESH,
                ).start()

            return carry

        lax.fori_loop(0, 2 * heads, step, 0, unroll=True)

    def scatter_done(send, slots, ss, rs):
        def step(k, carry):
            i = k // 2
            u = lax.rem(k, 2)
            chip = t * heads + i
            is_self = jnp.logical_and(chip == s, u == t)

            @pl.when(jnp.logical_not(is_self))
            def _():
                pltpu.make_async_remote_copy(
                    src_ref=send.at[i, u], dst_ref=slots(u), send_sem=ss.at[i, u], recv_sem=rs.at[s],
                    device_id={"sp": chip, "tp": u}, device_id_type=MESH,
                ).wait_send()

            return carry

        lax.fori_loop(0, 2 * heads, step, 0)

    kv_slot = lambda u: kv_all.at[s, u]
    q_slot = lambda u: q_all.at[s]
    scatter(kv_send, kv_slot, kv_ss, kv_rs)

    l_qs.wait()
    queries = dot(normed[...], vqs[...])
    for i in range(heads):
        cols = slice(i * hd, (i + 1) * hd)
        for u in range(2):
            top = queries[u * half : u * half + quarter, cols]
            low = queries[u * half + quarter : (u + 1) * half, cols]
            q_send[i, u] = jnp.concatenate([top, low], axis=1).astype(bf)
    scatter(q_send, q_slot, q_ss, q_rs)

    l_kw.wait()
    kvw[:, : kv_heads * hd] = dot(normed[...], vkw[...]).astype(bf)
    l_vw.wait()
    kvw[:, kv_heads * hd :] = dot(normed[...], vvw[...]).astype(bf)
    prev_copy = lambda to: pltpu.make_async_remote_copy(
        src_ref=kvw, dst_ref=kvw_prev, send_sem=p_ss, recv_sem=p_rs,
        device_id={"sp": to, "tp": t}, device_id_type=MESH,
    )

    l_qw.wait()
    qw = dot(normed[...], vqw[...])

    def forward(k, carry):
        src = k
        pltpu.make_async_remote_copy(
            src_ref=kv_send.at[0, 0], dst_ref=kv_all.at[src, t], send_sem=kv_ss.at[0, 0],
            recv_sem=kv_rs.at[src], device_id={"sp": s, "tp": other}, device_id_type=MESH,
        ).wait_recv()
        to_partner(kv_all.at[src, t], kv_all.at[src, t], f_ss.at[src], f_rs.at[src]).start()
        return carry

    def forward_arrived(k, carry):
        to_partner(kv_all.at[k, other], kv_all.at[k, other], f_ss.at[k], f_rs.at[k]).wait_recv()
        return carry

    def forward_sent(k, carry):
        to_partner(kv_all.at[k, t], kv_all.at[k, t], f_ss.at[k], f_rs.at[k]).wait_send()
        return carry

    def take_q(k, carry):
        pltpu.make_async_remote_copy(
            src_ref=q_send.at[0, 0], dst_ref=q_all.at[k], send_sem=q_ss.at[0, 0],
            recv_sem=q_rs.at[k], device_id={"sp": s, "tp": other}, device_id_type=MESH,
        ).wait_recv()
        slab = q_all[k].astype(f32)
        zero = jnp.zeros((quarter, hd), f32)
        both = jnp.concatenate(
            [
                jnp.concatenate([slab[:, :hd], zero], axis=1),
                jnp.concatenate([slab[:, hd:], zero], axis=1),
            ],
            axis=0,
        )
        q_pad[pl.ds(pl.multiple_of(k * half, half), half), :] = both.astype(bf)
        return carry

    b_copy.wait_recv()
    head_bias = bias_buf[s // heads, pl.ds(lax.rem(s, heads), 1), :][:, :1]

    kt = 2 * rows
    chunk = 4 * half
    later = (
        lax.broadcasted_iota(jnp.int32, (kt, kt), 0) > lax.broadcasted_iota(jnp.int32, (kt, kt), 1)
    ).astype(bf)
    row = lax.broadcasted_iota(jnp.int32, (chunk, kt), 0)
    lane = lax.broadcasted_iota(jnp.int32, (chunk, kt), 1)
    q_at = (row // half) * rows + t * half + lax.rem(row, half)
    scale = LOG2E * hd**-0.5

    def tile_of(n):
        return kv_all[2 * n : 2 * n + 2].reshape(kt, 2 * hd)

    owner = s // heads
    slot = lax.rem(s, heads)
    n_chunks = n_sp // 4

    def arrive(qc):
        lax.fori_loop(qc * 4, qc * 4 + 4, forward, 0, unroll=True)
        lax.fori_loop(qc * 4, qc * 4 + 4, take_q, 0, unroll=True)

    arrive(0)
    for qc in range(n_chunks):
        if qc + 1 < n_chunks:
            arrive(qc + 1)
        if qc + 2 == n_chunks:
            @pl.when(s < n_sp - 1)
            def _():
                prev_copy(s + 1).start()

        lax.fori_loop(qc * 4, qc * 4 + 4, forward_arrived, 0, unroll=True)
        last = 2 * qc + 1
        carry = jnp.zeros((chunk, 1), f32)
        carries = {}
        for n in range(last, -1, -1):
            low = chunk // 2 if n == last else 0
            qs = q_pad[qc * chunk + low : (qc + 1) * chunk, :]
            z = dot_t(qs, tile_of(n)) * scale + head_bias
            pos = jnp.maximum(z, 0.0)
            neg = z - pos
            soft = jnp.log2(1.0 + jnp.exp2(neg - pos))
            drop = pos + soft
            hold = neg - soft
            if n >= last - 1:
                usable = (lane + (n - 2 * qc) * kt < q_at)[low:]
                drop = jnp.where(usable, drop, 0.0)
                hold = jnp.where(usable, hold, -jnp.inf)
            suffix = dot(drop.astype(bf), later)
            staged[low:, n * kt : (n + 1) * kt] = hold - suffix
            carries[n] = carry[low:]
            step = suffix[:, :1] + drop[:, :1]
            if low:
                step = jnp.concatenate([jnp.zeros((low, 1), f32), step], axis=0)
            carry = carry + step
        acc = None
        for n in range(last - 1, -1, -1):
            weights = jnp.exp2(staged[:, n * kt : (n + 1) * kt] - carries[n]).astype(bf)
            res = dot(weights, tile_of(n))
            acc = res if acc is None else acc + res
        low = chunk // 2
        weights = jnp.exp2(staged[low:, last * kt : (last + 1) * kt] - carries[last]).astype(bf)
        tail = dot(weights, tile_of(last))
        acc = jnp.concatenate([acc[:low], acc[low:] + tail], axis=0)
        for b in range(4):
            top = acc[b * half : b * half + quarter, hd:]
            bot = acc[b * half + quarter : (b + 1) * half, hd:]
            o_send[qc * 4 + b] = jnp.concatenate([top, bot], axis=1).astype(bf)

        def give(k, carry):
            is_self = jnp.logical_and(k == s, t == owner)

            @pl.when(is_self)
            def _():
                pltpu.make_async_copy(o_send.at[k], o_recv.at[slot, t], o_rs.at[slot, t]).start()

            @pl.when(jnp.logical_not(is_self))
            def _():
                pltpu.make_async_remote_copy(
                    src_ref=o_send.at[k], dst_ref=o_recv.at[slot, t], send_sem=o_ss.at[k],
                    recv_sem=o_rs.at[slot, t], device_id={"sp": k, "tp": owner}, device_id_type=MESH,
                ).start()

            return carry

        lax.fori_loop(qc * 4, qc * 4 + 4, give, 0)

    @pl.when(s == 0)
    def _():
        kvw_prev[...] = jnp.zeros_like(kvw_prev)

    @pl.when(s > 0)
    def _():
        prev_copy(s - 1).wait_recv()

    two = 2 * rows
    r_iota = lax.broadcasted_iota(jnp.int32, (two, two), 0)
    c_iota = lax.broadcasted_iota(jnp.int32, (two, two), 1)
    dist = lax.rem(r_iota, rows) + rows - c_iota
    in_window = (dist >= 0) & (dist < WINDOW) & ((c_iota >= rows) | (s > 0))
    first_rows = lax.broadcasted_iota(jnp.int32, (two, 1), 0) < rows
    for g in range(kv_heads):
        cols = slice(g * hd, (g + 1) * hd)
        v_cols = slice((kv_heads + g) * hd, (kv_heads + g + 1) * hd)
        kk = jnp.concatenate([kvw_prev[:, cols], kvw[:, cols]], axis=0)
        vv = jnp.concatenate([kvw_prev[:, v_cols], kvw[:, v_cols]], axis=0)
        base = g * GROUP * hd
        qq = jnp.concatenate(
            [qw[:, base : base + hd], qw[:, base + hd : base + 2 * hd]], axis=0
        ).astype(bf)
        logits = jnp.where(in_window, dot_t(qq, kk) * hd**-0.5, -jnp.inf)
        sink = jnp.where(first_rows, sinks[GROUP * g], sinks[GROUP * g + 1])
        top = jnp.maximum(jnp.max(logits, axis=1, keepdims=True), sink)
        grown = jnp.exp(logits - top)
        total = jnp.sum(grown, axis=1, keepdims=True) + jnp.exp(sink - top)
        weights = (grown / total).astype(bf)
        res = dot(weights, vv)
        w_out_buf[:, base : base + 2 * hd] = jnp.concatenate([res[:rows], res[rows:]], axis=1).astype(bf)

    wf = w_out_buf[...].astype(f32)
    sq_send[0] = jnp.broadcast_to(jnp.sum(wf * wf, axis=1, keepdims=True), (rows, 128))

    sq_w = to_partner(sq_send.at[0], sq_recv.at[0], sq_ss.at[0], sq_rs.at[0])
    sq_w.start()

    l_ow.wait()
    total_w[...] = dot((wf * wgain[...].reshape(1, sw)).astype(bf), vow[...])
    sq_w.wait_recv()
    sw_cols = 2.0 * sw
    inv_w = lax.rsqrt((sq_send[0] + sq_recv[0])[:, :1] / sw_cols + EPS)

    def take_o(k, carry):
        pltpu.make_async_remote_copy(
            src_ref=o_send.at[0], dst_ref=o_recv.at[k // 2, lax.rem(k, 2)], send_sem=o_ss.at[0],
            recv_sem=o_rs.at[k // 2, lax.rem(k, 2)], device_id={"sp": s, "tp": other}, device_id_type=MESH,
        ).wait_recv()
        return carry

    lax.fori_loop(0, 2 * heads, take_o, 0)
    for j in range(heads // 2):
        for u in range(2):
            one = o_recv[2 * j, u].astype(f32)
            two_ = o_recv[2 * j + 1, u].astype(f32)
            s_out_buf[u * half : u * half + quarter, 2 * j * hd : 2 * (j + 1) * hd] = jnp.concatenate(
                [one[:, :hd], two_[:, :hd]], axis=1
            )
            s_out_buf[u * half + quarter : (u + 1) * half, 2 * j * hd : 2 * (j + 1) * hd] = jnp.concatenate(
                [one[:, hd:], two_[:, hd:]], axis=1
            )
    sf = s_out_buf[...]
    sq_send[1] = jnp.broadcast_to(jnp.sum(sf * sf, axis=1, keepdims=True), (rows, 128))
    gained = (sf * sgain[...].reshape(1, sw)).astype(bf)
    sq_s = to_partner(sq_send.at[1], sq_recv.at[1], sq_ss.at[1], sq_rs.at[1])
    sq_s.start()
    l_os.wait()
    n_cut = c_send.shape[0]
    cut = feats // n_cut
    for n in range(n_cut):
        comb[:, n * cut : (n + 1) * cut] = dot(gained, vos[:, n * cut : (n + 1) * cut])
    sq_s.wait_recv()
    inv_s = lax.rsqrt((sq_send[1] + sq_recv[1])[:, :1] / sw_cols + EPS)
    copies = []
    theirs = pl.ds(pl.multiple_of(other * half, half), half)
    mine = pl.ds(pl.multiple_of(t * half, half), half)
    for n in range(n_cut):
        cols = slice(n * cut, (n + 1) * cut)
        comb[:, cols] = comb[:, cols] * inv_s + total_w[:, cols] * inv_w
        c_send[n] = comb[theirs, cols].astype(bf)
        copy = to_partner(c_send.at[n], c_recv.at[n], c_ss.at[n], c_rs.at[n])
        copy.start()
        copies.append(copy)
    square = jnp.zeros((half, 1), f32)
    for n in range(n_cut):
        cols = slice(n * cut, (n + 1) * cut)
        copies[n].wait_recv()
        summed = (comb[mine, cols] + c_recv[n].astype(f32)).astype(bf).astype(f32)
        total_w[:half, cols] = summed
        square = square + jnp.sum(summed * summed, axis=1, keepdims=True)
    inv = lax.rsqrt(square / feats + EPS)
    out[...] = (total_w[:half, :] * inv * post_gain[...].reshape(1, feats)).astype(bf)

    x_copy.wait_send()
    b_copy.wait_send()
    scatter_done(kv_send, kv_slot, kv_ss, kv_rs)
    scatter_done(q_send, q_slot, q_ss, q_rs)
    lax.fori_loop(0, n_sp, forward_sent, 0)

    @pl.when(s < n_sp - 1)
    def _():
        prev_copy(s + 1).wait_send()

    def gave(k, carry):
        @pl.when(jnp.logical_not(jnp.logical_and(k == s, t == owner)))
        def _():
            pltpu.make_async_remote_copy(
                src_ref=o_send.at[k], dst_ref=o_recv.at[slot, t], send_sem=o_ss.at[k],
                recv_sem=o_rs.at[slot, t], device_id={"sp": k, "tp": owner}, device_id_type=MESH,
            ).wait_send()

        return carry

    lax.fori_loop(0, n_sp, gave, 0)
    sq_w.wait_send()
    sq_s.wait_send()
    for copy in copies:
        copy.wait_send()


def one_kernel(n_sp, *args):
    tokens, pre_gain, wqs, wks, wvs, wqw, wkw, wvw, bias, sinks, sgain, wgain, wos, wow, post_gain = args
    bf = jnp.bfloat16
    f32 = jnp.float32
    rows, feat_half = tokens.shape
    feats = 2 * feat_half
    half = rows // 2
    hd = HEAD_DIM
    heads = wqs.shape[1] // hd
    sw = wqs.shape[1]
    wide = 2 * hd
    kvw_cols = wkw.shape[1] + wvw.shape[1]
    assert 2 * heads == n_sp and rows == WINDOW
    v = pltpu.VMEM
    dma = pltpu.SemaphoreType.DMA
    anywhere = pl.BlockSpec(memory_space=pl.ANY)
    vmem = pl.BlockSpec(memory_space=pltpu.VMEM)
    n_cut = 4
    scratch = [
        v(pre_gain.shape, f32), pltpu.SMEM(bias.shape, f32), pltpu.SMEM(sinks.shape, f32),
        v(sgain.shape, f32), v(wgain.shape, f32), v(post_gain.shape, f32),
        v((2, rows, feat_half), bf), v((2, heads, 128), f32), v((rows, feats), bf),
        v(wqs.shape, bf), v(wks.shape, bf), v(wvs.shape, bf), v(wqw.shape, bf), v(wkw.shape, bf),
        v(wvw.shape, bf), v(wos.shape, bf), v(wow.shape, bf),
        v((heads, 2, half, wide), bf), v((heads, 2, half // 2, wide), bf),
        v((n_sp, 2, half, wide), bf), v((n_sp, half // 2, wide), bf),
        v((n_sp * half, wide), bf), v((4 * half, n_sp * rows), f32),
        v((rows, kvw_cols), bf), v((rows, kvw_cols), bf), v((rows, sw), bf),
        v((n_sp, half // 2, wide), bf), v((heads, 2, half // 2, wide), bf), v((rows, sw), f32),
        v((2, rows, 128), f32), v((2, rows, 128), f32), v((rows, feats), f32), v((rows, feats), f32),
        v((n_cut, half, feats // n_cut), bf), v((n_cut, half, feats // n_cut), bf),
        dma((14,)), dma, dma, dma, dma, dma, dma((heads, 2)), dma((n_sp,)), dma((heads, 2)), dma((n_sp,)),
        dma((n_sp,)), dma((n_sp,)), dma, dma, dma((n_sp,)), dma((heads, 2)), dma((2,)), dma((2,)),
        dma((n_cut,)), dma((n_cut,)),
    ]
    return pl.pallas_call(
        functools.partial(kernel, n_sp),
        out_shape=jax.ShapeDtypeStruct((half, feats), bf),
        in_specs=[anywhere] * len(args),
        out_specs=vmem,
        scratch_shapes=scratch,
        compiler_params=pltpu.CompilerParams(
            collective_id=0, has_side_effects=True, vmem_limit_bytes=67043328
        ),
        name="layer",
    )(*args)


def passed_along(value, axis, steps):
    count = lax.axis_size(axis)
    initial, last = (max(0, -steps), min(count, count - steps))
    return lax.ppermute(value, axis, [(source, source + steps) for source in range(initial, last)])


def rounded(values):
    return lax.optimization_barrier(values.astype(jnp.bfloat16)).astype(jnp.float32)


def norm_rows(values, gain):
    stats = jnp.mean(values * values, axis=-1, keepdims=True)
    return values * lax.rsqrt(stats + EPS) * gain


def stick_block(queries, key_pair, head_bias, key_mask, carried):
    result, logsum = carried
    head_count = queries.shape[1]
    key_rows = key_pair[0].reshape(key_pair.shape[1], head_count, HEAD_DIM)
    values = key_pair[1].reshape(key_pair.shape[1], head_count, HEAD_DIM)
    scores = jnp.einsum(
        "thd,shd->hts", queries, key_rows, preferred_element_type=jnp.float32
    ) * HEAD_DIM ** (-0.5)
    scores = scores + head_bias[:, None, None]
    usable = key_mask[None]
    log_keep = jnp.where(usable, jax.nn.log_sigmoid(-scores), 0.0)
    suffix = lax.cumsum(log_keep, axis=2, reverse=True) - log_keep
    stick_weights = jnp.where(
        usable, jnp.exp(jax.nn.log_sigmoid(scores) + suffix + logsum[:, :, None]), 0.0
    )
    stick_weights = stick_weights.astype(jnp.bfloat16)
    result = result + jnp.einsum(
        "hts,shd->htd", stick_weights, values, preferred_element_type=jnp.float32
    )
    logsum = logsum + jnp.sum(log_keep, axis=2)
    return (result, logsum)


def by_collectives(
    tokens,
    pre_gain,
    w_query_stick,
    w_key_stick,
    w_value_stick,
    w_query_window,
    w_key_window,
    w_value_window,
    stick_bias,
    sinks,
    stick_gain,
    window_gain,
    w_out_stick,
    w_out_window,
    post_gain,
):
    gathered = lax.all_gather(tokens, "tp", axis=1, tiled=True)
    normed = norm_rows(gathered.astype(jnp.float32), pre_gain).astype(jnp.bfloat16)

    def project(weight):
        return jnp.dot(normed, weight, preferred_element_type=jnp.float32).astype(jnp.bfloat16)

    tok_rows = normed.shape[0]
    dev_index = lax.axis_index("sp")
    dev_count = lax.axis_size("sp")
    query_stick = project(w_query_stick)
    stick_heads = query_stick.shape[1] // HEAD_DIM
    queries = query_stick.reshape(tok_rows, stick_heads, HEAD_DIM)
    own_pair = jnp.stack([project(w_key_stick), project(w_value_stick)])
    pair_width = own_pair.shape[2]
    positions = jnp.arange(tok_rows, dtype=jnp.int32)
    initial = (
        jnp.zeros((stick_heads, tok_rows, HEAD_DIM), jnp.float32),
        jnp.zeros((stick_heads, tok_rows), jnp.float32),
    )
    collected = own_pair[None]
    for section_index in range(dev_count.bit_length() - 1):
        arrived = passed_along(collected, "sp", 2**section_index)
        collected = jnp.concatenate([arrived, collected], axis=0)
    per_group = min(dev_count, 8)
    group_count = dev_count // per_group
    grouped = collected.reshape(group_count, per_group, 2, tok_rows, pair_width)
    grouped = grouped.transpose(0, 2, 1, 3, 4).reshape(
        group_count, 2, per_group * tok_rows, pair_width
    )
    first_source = dev_index - (dev_count - 1)
    group_starts = (first_source + jnp.arange(group_count, dtype=jnp.int32) * per_group) * tok_rows
    query_pos = dev_index * tok_rows + positions
    span_offs = jnp.arange(per_group * tok_rows, dtype=jnp.int32)

    def visit_group(carried, inputs):
        key_pair, start_pos = inputs
        key_pos = start_pos + span_offs
        key_mask = (key_pos[None, :] >= 0) & (key_pos[None, :] < query_pos[:, None])
        return (stick_block(queries, key_pair, stick_bias, key_mask, carried), None)

    (stick_sum, _), _ = lax.scan(visit_group, initial, (grouped, group_starts), reverse=True)
    stick_out = (
        stick_sum.transpose(1, 0, 2).reshape(tok_rows, stick_heads * HEAD_DIM).astype(jnp.bfloat16)
    )
    query_window = project(w_query_window)
    window_pair = jnp.stack([project(w_key_window), project(w_value_window)])
    kv_heads = window_pair.shape[2] // HEAD_DIM
    previous = passed_along(window_pair, "sp", 1)
    extended = jnp.concatenate([previous, window_pair], axis=1)
    block_count = tok_rows // WINDOW
    extended = extended.reshape(2, block_count + 1, WINDOW, kv_heads, HEAD_DIM)
    banded = jnp.concatenate([extended[:, :-1], extended[:, 1:]], axis=2)
    q_blocks = query_window.reshape(block_count, WINDOW, kv_heads, GROUP, HEAD_DIM)
    logits = jnp.einsum(
        "nqhgd,nchd->nhgqc", q_blocks, banded[0], preferred_element_type=jnp.float32
    ) * HEAD_DIM ** (-0.5)
    query_offs = jnp.arange(WINDOW, dtype=jnp.int32)[:, None]
    key_offs = jnp.arange(2 * WINDOW, dtype=jnp.int32)[None, :]
    distance = query_offs + WINDOW - key_offs
    key_pos = (
        dev_index * tok_rows
        + jnp.arange(block_count, dtype=jnp.int32)[:, None] * WINDOW
        - WINDOW
        + key_offs
    )
    usable = ((distance >= 0) & (distance < WINDOW))[None] & (key_pos >= 0)[:, None, :]
    logits = jnp.where(usable[:, None, None], logits, -jnp.inf)
    sink_logit = sinks.reshape(kv_heads, GROUP)[None, :, :, None, None]
    row_top = jnp.maximum(jnp.max(logits, axis=-1, keepdims=True), sink_logit)
    weights_exp = jnp.exp(logits - row_top)
    normalizer = jnp.sum(weights_exp, axis=-1, keepdims=True) + jnp.exp(sink_logit - row_top)
    window_weights = (weights_exp / normalizer).astype(jnp.bfloat16)
    window_sum = jnp.einsum(
        "nhgqc,nchd->nqhgd", window_weights, banded[1], preferred_element_type=jnp.float32
    )
    window_out = window_sum.reshape(tok_rows, query_window.shape[1]).astype(jnp.bfloat16)
    stick_float = stick_out.astype(jnp.float32)
    window_float = window_out.astype(jnp.float32)
    squares = lax.psum(
        (jnp.sum(stick_float * stick_float, axis=1), jnp.sum(window_float * window_float, axis=1)),
        "tp",
    )
    stick_normed = (
        stick_float * lax.rsqrt(squares[0][:, None] / (stick_gain.shape[0] * lax.axis_size("tp")) + EPS) * stick_gain
    ).astype(jnp.bfloat16)
    window_normed = (
        window_float * lax.rsqrt(squares[1][:, None] / (window_gain.shape[0] * lax.axis_size("tp")) + EPS) * window_gain
    ).astype(jnp.bfloat16)
    total = jnp.dot(stick_normed, w_out_stick, preferred_element_type=jnp.float32)
    combined = lax.psum_scatter(
        (total + jnp.dot(window_normed, w_out_window, preferred_element_type=jnp.float32)).astype(
            jnp.bfloat16
        ),
        "tp",
        scatter_dimension=0,
        tiled=True,
    ).astype(jnp.float32)
    combined = rounded(combined)
    return norm_rows(combined, post_gain).astype(jnp.bfloat16)


def solution(mesh):
    in_specs = (
        P("sp", "tp"),
        P(),
        P(None, "tp"),
        P(None, "tp"),
        P(None, "tp"),
        P(None, "tp"),
        P(None, "tp"),
        P(None, "tp"),
        P("tp"),
        P("tp"),
        P("tp"),
        P("tp"),
        P("tp", None),
        P("tp", None),
        P(),
    )
    n_sp, n_tp = mesh.shape["sp"], mesh.shape["tp"]

    def shards(*args):
        heads = args[2].shape[1] // HEAD_DIM
        if n_tp == 2 and n_tp * heads == n_sp and args[0].shape[0] == WINDOW and n_sp % 4 == 0:
            return one_kernel(n_sp, *args)
        return by_collectives(*args)

    return jax.shard_map(
        shards,
        mesh=mesh,
        in_specs=in_specs,
        out_specs=P(("sp", "tp"), None),
        check_vma=False,
    )
```

```python
import functools

import jax
import jax.numpy as jnp
from jax import lax
from jax.experimental import pallas as pl
from jax.experimental.pallas import tpu as pltpu
from jax.sharding import PartitionSpec as P

HEAD_DIM = 64
GROUP = 2
WINDOW = 128
EPS = 1e-06
LOG2E = 1.4426950408889634
MESH = pl.DeviceIdType.MESH


def dot(a, b):
    return jnp.dot(a, b, preferred_element_type=jnp.float32)


def dot_t(a, b):
    return lax.dot_general(a, b, (((1,), (1,)), ((), ())), preferred_element_type=jnp.float32)


def kernel(
    n_sp,
    tokens, pre_gain_in, wqs, wks, wvs, wqw, wkw, wvw, bias_in, sinks_in, sgain_in, wgain_in, wos, wow,
    post_gain_in, out,
    pre_gain, bias, sinks, sgain, wgain, post_gain, x, bias_buf, normed, vqs, vks, vvs, vqw, vkw, vvw, vos, vow,
    kv_send, kv_all, q_pad, staged,
    kvw, kvw_prev, w_out_buf, o_send, o_recv, s_out_buf,
    sq_send, sq_recv, total_w, comb, c_send, c_recv,
    w_sem, tok_sem, x_ss, x_rs, b_ss, b_rs, kv_ss, kv_rs, f_ss, f_rs,
    p_ss, p_rs, o_ss, o_rs, sq_ss, sq_rs, c_ss, c_rs,
):
    bf = jnp.bfloat16
    f32 = jnp.float32
    s = lax.axis_index("sp")
    t = lax.axis_index("tp")
    other = 1 - t
    rows, feat_half = tokens.shape
    feats = 2 * feat_half
    half = rows // 2
    quarter = half // 2
    hd = HEAD_DIM
    heads = wqs.shape[1] // hd
    kv_heads = wkw.shape[1] // hd
    sw = wqs.shape[1]

    barrier = pltpu.get_barrier_semaphore()
    me = s * 2 + t

    def greet(k, carry):
        peer = lax.rem(me + k, 2 * n_sp)
        pl.semaphore_signal(
            barrier, inc=1, device_id={"sp": peer // 2, "tp": lax.rem(peer, 2)}, device_id_type=MESH
        )
        return carry

    lax.fori_loop(1, 2 * n_sp, greet, 0)

    loads = [
        pltpu.make_async_copy(src, dst, w_sem.at[n])
        for n, (src, dst) in enumerate(
            [(wks, vks), (wvs, vvs), (wqs, vqs), (wkw, vkw), (wvw, vvw), (wqw, vqw), (wow, vow), (wos, vos),
             (bias_in, bias), (pre_gain_in, pre_gain), (sinks_in, sinks), (sgain_in, sgain),
             (wgain_in, wgain), (post_gain_in, post_gain)]
        )
    ]
    l_ks, l_vs, l_qs, l_kw, l_vw, l_qw, l_ow, l_os, l_bias, *l_small = loads
    tok_load = pltpu.make_async_copy(tokens, x.at[t], tok_sem)
    l_bias.start()
    tok_load.start()
    for load in l_small + loads[:8]:
        load.start()

    row_id = lax.broadcasted_iota(jnp.int32, (heads, 128), 0)
    bias_rows = jnp.zeros((heads, 128), f32)
    l_bias.wait()
    for i in range(heads):
        bias_rows = jnp.where(row_id == i, bias[i] * LOG2E, bias_rows)
    bias_buf[t] = bias_rows

    for load in l_small:
        load.wait()
    tok_load.wait()
    pl.semaphore_wait(barrier, 2 * n_sp - 1)

    def to_partner(src, dst, ss, rs):
        return pltpu.make_async_remote_copy(
            src_ref=src, dst_ref=dst, send_sem=ss, recv_sem=rs,
            device_id={"sp": s, "tp": other}, device_id_type=MESH,
        )

    x_copy = to_partner(x.at[t], x.at[t], x_ss, x_rs)
    b_copy = to_partner(bias_buf.at[t], bias_buf.at[t], b_ss, b_rs)
    x_copy.start()
    b_copy.start()
    x_copy.wait_recv()

    gain = pre_gain[...].reshape(1, feats)

    def norm_step(n, carry):
        part = pl.ds(pl.multiple_of(n * 32, 32), 32)
        left = x[0, part, :].astype(f32)
        right = x[1, part, :].astype(f32)
        stats = (
            jnp.sum(left * left, axis=1, keepdims=True) + jnp.sum(right * right, axis=1, keepdims=True)
        ) * (1.0 / feats)
        inv = lax.rsqrt(stats + EPS)
        normed[part, :feat_half] = (left * inv * gain[:, :feat_half]).astype(bf)
        normed[part, feat_half:] = (right * inv * gain[:, feat_half:]).astype(bf)
        return carry

    lax.fori_loop(0, rows // 32, norm_step, 0)

    l_ks.wait()
    keys = dot(normed[...], vks[...])
    l_vs.wait()
    values = dot(normed[...], vvs[...])
    for i in range(heads):
        cols = slice(i * hd, (i + 1) * hd)
        packed = jnp.concatenate([keys[:, cols], values[:, cols]], axis=1).astype(bf)
        kv_send[i, :, :half] = packed.reshape(2, half, 2 * hd)

    def scatter(send, slots, ss, rs):
        def step(k, carry):
            i = lax.rem(k // 2 + s, heads)
            u = lax.rem(k, 2)
            chip = t * heads + i
            is_self = jnp.logical_and(chip == s, u == t)

            @pl.when(is_self)
            def _():
                pltpu.make_async_copy(send.at[i, u], slots(u), rs.at[s]).start()

            @pl.when(jnp.logical_not(is_self))
            def _():
                pltpu.make_async_remote_copy(
                    src_ref=send.at[i, u], dst_ref=slots(u), send_sem=ss.at[i, u], recv_sem=rs.at[s],
                    device_id={"sp": chip, "tp": u}, device_id_type=MESH,
                ).start()

            return carry

        lax.fori_loop(0, 2 * heads, step, 0, unroll=True)

    def scatter_done(send, slots, ss, rs):
        def step(k, carry):
            i = k // 2
            u = lax.rem(k, 2)
            chip = t * heads + i
            is_self = jnp.logical_and(chip == s, u == t)

            @pl.when(jnp.logical_not(is_self))
            def _():
                pltpu.make_async_remote_copy(
                    src_ref=send.at[i, u], dst_ref=slots(u), send_sem=ss.at[i, u], recv_sem=rs.at[s],
                    device_id={"sp": chip, "tp": u}, device_id_type=MESH,
                ).wait_send()

            return carry

        lax.fori_loop(0, 2 * heads, step, 0)

    kv_slot = lambda u: kv_all.at[s, u]

    l_qs.wait()
    queries = dot(normed[...], vqs[...])
    for i in range(heads):
        cols = slice(i * hd, (i + 1) * hd)
        for u in range(2):
            top = queries[u * half : u * half + quarter, cols]
            low = queries[u * half + quarter : (u + 1) * half, cols]
            kv_send[i, u, half:] = jnp.concatenate([top, low], axis=1).astype(bf)
    scatter(kv_send, kv_slot, kv_ss, kv_rs)

    l_kw.wait()
    kvw[:, : kv_heads * hd] = dot(normed[...], vkw[...]).astype(bf)
    l_vw.wait()
    kvw[:, kv_heads * hd :] = dot(normed[...], vvw[...]).astype(bf)
    prev_copy = lambda to: pltpu.make_async_remote_copy(
        src_ref=kvw, dst_ref=kvw_prev, send_sem=p_ss, recv_sem=p_rs,
        device_id={"sp": to, "tp": t}, device_id_type=MESH,
    )

    l_qw.wait()
    qw = dot(normed[...], vqw[...])

    def forward(k, carry):
        src = k
        pltpu.make_async_remote_copy(
            src_ref=kv_send.at[0, 0], dst_ref=kv_all.at[src, t], send_sem=kv_ss.at[0, 0],
            recv_sem=kv_rs.at[src], device_id={"sp": s, "tp": other}, device_id_type=MESH,
        ).wait_recv()
        to_partner(kv_all.at[src, t, :half], kv_all.at[src, t, :half], f_ss.at[src], f_rs.at[src]).start()
        return carry

    def forward_arrived(k, carry):
        to_partner(kv_all.at[k, other, :half], kv_all.at[k, other, :half], f_ss.at[k], f_rs.at[k]).wait_recv()
        return carry

    def forward_sent(k, carry):
        to_partner(kv_all.at[k, t, :half], kv_all.at[k, t, :half], f_ss.at[k], f_rs.at[k]).wait_send()
        return carry

    def take_q(k, carry):
        slab = kv_all[k, t, half:].astype(f32)
        zero = jnp.zeros((quarter, hd), f32)
        both = jnp.concatenate(
            [
                jnp.concatenate([slab[:, :hd], zero], axis=1),
                jnp.concatenate([slab[:, hd:], zero], axis=1),
            ],
            axis=0,
        )
        q_pad[pl.ds(pl.multiple_of(k * half, half), half), :] = both.astype(bf)
        return carry

    b_copy.wait_recv()
    head_bias = bias_buf[s // heads, pl.ds(lax.rem(s, heads), 1), :][:, :1]

    kt = 2 * rows
    chunk = 4 * half
    later = (
        lax.broadcasted_iota(jnp.int32, (kt, kt), 0) > lax.broadcasted_iota(jnp.int32, (kt, kt), 1)
    ).astype(bf)
    row = lax.broadcasted_iota(jnp.int32, (chunk, kt), 0)
    lane = lax.broadcasted_iota(jnp.int32, (chunk, kt), 1)
    q_at = (row // half) * rows + t * half + lax.rem(row, half)
    scale = LOG2E * hd**-0.5

    def tile_of(n):
        return kv_all[2 * n : 2 * n + 2, :, :half].reshape(kt, 2 * hd)

    owner = s // heads
    slot = lax.rem(s, heads)
    n_chunks = n_sp // 4

    def arrive(qc):
        lax.fori_loop(qc * 4, qc * 4 + 4, forward, 0, unroll=True)
        lax.fori_loop(qc * 4, qc * 4 + 4, take_q, 0, unroll=True)

    arrive(0)
    for qc in range(n_chunks):
        if qc + 1 < n_chunks:
            arrive(qc + 1)
        if qc + 2 == n_chunks:
            @pl.when(s < n_sp - 1)
            def _():
                prev_copy(s + 1).start()

        lax.fori_loop(qc * 4, qc * 4 + 4, forward_arrived, 0, unroll=True)
        last = 2 * qc + 1
        carry = jnp.zeros((chunk, 1), f32)
        carries = {}
        for n in range(last, -1, -1):
            low = chunk // 2 if n == last else 0
            qs = q_pad[qc * chunk + low : (qc + 1) * chunk, :]
            z = dot_t(qs, tile_of(n)) * scale + head_bias
            pos = jnp.maximum(z, 0.0)
            neg = z - pos
            soft = jnp.log2(1.0 + jnp.exp2(neg - pos))
            drop = pos + soft
            hold = neg - soft
            if n >= last - 1:
                usable = (lane + (n - 2 * qc) * kt < q_at)[low:]
                drop = jnp.where(usable, drop, 0.0)
                hold = jnp.where(usable, hold, -jnp.inf)
            suffix = dot(drop.astype(bf), later)
            staged[low:, n * kt : (n + 1) * kt] = hold - suffix
            carries[n] = carry[low:]
            step = suffix[:, :1] + drop[:, :1]
            if low:
                step = jnp.concatenate([jnp.zeros((low, 1), f32), step], axis=0)
            carry = carry + step
        acc = None
        for n in range(last - 1, -1, -1):
            weights = jnp.exp2(staged[:, n * kt : (n + 1) * kt] - carries[n]).astype(bf)
            res = dot(weights, tile_of(n))
            acc = res if acc is None else acc + res
        low = chunk // 2
        weights = jnp.exp2(staged[low:, last * kt : (last + 1) * kt] - carries[last]).astype(bf)
        tail = dot(weights, tile_of(last))
        acc = jnp.concatenate([acc[:low], acc[low:] + tail], axis=0)
        for b in range(4):
            top = acc[b * half : b * half + quarter, hd:]
            bot = acc[b * half + quarter : (b + 1) * half, hd:]
            o_send[qc * 4 + b] = jnp.concatenate([top, bot], axis=1).astype(bf)

        def give(k, carry):
            is_self = jnp.logical_and(k == s, t == owner)

            @pl.when(is_self)
            def _():
                pltpu.make_async_copy(o_send.at[k], o_recv.at[slot, t], o_rs.at[slot, t]).start()

            @pl.when(jnp.logical_not(is_self))
            def _():
                pltpu.make_async_remote_copy(
                    src_ref=o_send.at[k], dst_ref=o_recv.at[slot, t], send_sem=o_ss.at[k],
                    recv_sem=o_rs.at[slot, t], device_id={"sp": k, "tp": owner}, device_id_type=MESH,
                ).start()

            return carry

        lax.fori_loop(qc * 4, qc * 4 + 4, give, 0)

    @pl.when(s == 0)
    def _():
        kvw_prev[...] = jnp.zeros_like(kvw_prev)

    @pl.when(s > 0)
    def _():
        prev_copy(s - 1).wait_recv()

    two = 2 * rows
    r_iota = lax.broadcasted_iota(jnp.int32, (two, two), 0)
    c_iota = lax.broadcasted_iota(jnp.int32, (two, two), 1)
    dist = lax.rem(r_iota, rows) + rows - c_iota
    in_window = (dist >= 0) & (dist < WINDOW) & ((c_iota >= rows) | (s > 0))
    first_rows = lax.broadcasted_iota(jnp.int32, (two, 1), 0) < rows
    for g in range(kv_heads):
        cols = slice(g * hd, (g + 1) * hd)
        v_cols = slice((kv_heads + g) * hd, (kv_heads + g + 1) * hd)
        kk = jnp.concatenate([kvw_prev[:, cols], kvw[:, cols]], axis=0)
        vv = jnp.concatenate([kvw_prev[:, v_cols], kvw[:, v_cols]], axis=0)
        base = g * GROUP * hd
        qq = jnp.concatenate(
            [qw[:, base : base + hd], qw[:, base + hd : base + 2 * hd]], axis=0
        ).astype(bf)
        logits = jnp.where(in_window, dot_t(qq, kk) * hd**-0.5, -jnp.inf)
        sink = jnp.where(first_rows, sinks[GROUP * g], sinks[GROUP * g + 1])
        top = jnp.maximum(jnp.max(logits, axis=1, keepdims=True), sink)
        grown = jnp.exp(logits - top)
        total = jnp.sum(grown, axis=1, keepdims=True) + jnp.exp(sink - top)
        weights = (grown / total).astype(bf)
        res = dot(weights, vv)
        w_out_buf[:, base : base + 2 * hd] = jnp.concatenate([res[:rows], res[rows:]], axis=1).astype(bf)

    wf = w_out_buf[...].astype(f32)
    sq_send[0] = jnp.broadcast_to(jnp.sum(wf * wf, axis=1, keepdims=True), (rows, 128))

    sq_w = to_partner(sq_send.at[0], sq_recv.at[0], sq_ss.at[0], sq_rs.at[0])
    sq_w.start()

    l_ow.wait()
    total_w[...] = dot((wf * wgain[...].reshape(1, sw)).astype(bf), vow[...])
    sq_w.wait_recv()
    sw_cols = 2.0 * sw
    inv_w = lax.rsqrt((sq_send[0] + sq_recv[0])[:, :1] / sw_cols + EPS)

    def take_o(k, carry):
        pltpu.make_async_remote_copy(
            src_ref=o_send.at[0], dst_ref=o_recv.at[k // 2, lax.rem(k, 2)], send_sem=o_ss.at[0],
            recv_sem=o_rs.at[k // 2, lax.rem(k, 2)], device_id={"sp": s, "tp": other}, device_id_type=MESH,
        ).wait_recv()
        return carry

    lax.fori_loop(0, 2 * heads, take_o, 0)
    for j in range(heads // 2):
        for u in range(2):
            one = o_recv[2 * j, u].astype(f32)
            two_ = o_recv[2 * j + 1, u].astype(f32)
            s_out_buf[u * half : u * half + quarter, 2 * j * hd : 2 * (j + 1) * hd] = jnp.concatenate(
                [one[:, :hd], two_[:, :hd]], axis=1
            )
            s_out_buf[u * half + quarter : (u + 1) * half, 2 * j * hd : 2 * (j + 1) * hd] = jnp.concatenate(
                [one[:, hd:], two_[:, hd:]], axis=1
            )
    sf = s_out_buf[...]
    sq_send[1] = jnp.broadcast_to(jnp.sum(sf * sf, axis=1, keepdims=True), (rows, 128))
    gained = (sf * sgain[...].reshape(1, sw)).astype(bf)
    sq_s = to_partner(sq_send.at[1], sq_recv.at[1], sq_ss.at[1], sq_rs.at[1])
    sq_s.start()
    l_os.wait()
    n_cut = c_send.shape[0]
    cut = feats // n_cut
    for n in range(n_cut):
        comb[:, n * cut : (n + 1) * cut] = dot(gained, vos[:, n * cut : (n + 1) * cut])
    sq_s.wait_recv()
    inv_s = lax.rsqrt((sq_send[1] + sq_recv[1])[:, :1] / sw_cols + EPS)
    copies = []
    theirs = pl.ds(pl.multiple_of(other * half, half), half)
    mine = pl.ds(pl.multiple_of(t * half, half), half)
    for n in range(n_cut):
        cols = slice(n * cut, (n + 1) * cut)
        comb[:, cols] = comb[:, cols] * inv_s + total_w[:, cols] * inv_w
        c_send[n] = comb[theirs, cols].astype(bf)
        copy = to_partner(c_send.at[n], c_recv.at[n], c_ss.at[n], c_rs.at[n])
        copy.start()
        copies.append(copy)
    square = jnp.zeros((half, 1), f32)
    for n in range(n_cut):
        cols = slice(n * cut, (n + 1) * cut)
        copies[n].wait_recv()
        summed = (comb[mine, cols] + c_recv[n].astype(f32)).astype(bf).astype(f32)
        total_w[:half, cols] = summed
        square = square + jnp.sum(summed * summed, axis=1, keepdims=True)
    inv = lax.rsqrt(square / feats + EPS)
    out[...] = (total_w[:half, :] * inv * post_gain[...].reshape(1, feats)).astype(bf)

    x_copy.wait_send()
    b_copy.wait_send()
    scatter_done(kv_send, kv_slot, kv_ss, kv_rs)
    lax.fori_loop(0, n_sp, forward_sent, 0)

    @pl.when(s < n_sp - 1)
    def _():
        prev_copy(s + 1).wait_send()

    def gave(k, carry):
        @pl.when(jnp.logical_not(jnp.logical_and(k == s, t == owner)))
        def _():
            pltpu.make_async_remote_copy(
                src_ref=o_send.at[k], dst_ref=o_recv.at[slot, t], send_sem=o_ss.at[k],
                recv_sem=o_rs.at[slot, t], device_id={"sp": k, "tp": owner}, device_id_type=MESH,
            ).wait_send()

        return carry

    lax.fori_loop(0, n_sp, gave, 0)
    sq_w.wait_send()
    sq_s.wait_send()
    for copy in copies:
        copy.wait_send()


def one_kernel(n_sp, *args):
    tokens, pre_gain, wqs, wks, wvs, wqw, wkw, wvw, bias, sinks, sgain, wgain, wos, wow, post_gain = args
    bf = jnp.bfloat16
    f32 = jnp.float32
    rows, feat_half = tokens.shape
    feats = 2 * feat_half
    half = rows // 2
    hd = HEAD_DIM
    heads = wqs.shape[1] // hd
    sw = wqs.shape[1]
    wide = 2 * hd
    kvw_cols = wkw.shape[1] + wvw.shape[1]
    assert 2 * heads == n_sp and rows == WINDOW
    v = pltpu.VMEM
    dma = pltpu.SemaphoreType.DMA
    anywhere = pl.BlockSpec(memory_space=pl.ANY)
    vmem = pl.BlockSpec(memory_space=pltpu.VMEM)
    n_cut = 4
    scratch = [
        v(pre_gain.shape, f32), pltpu.SMEM(bias.shape, f32), pltpu.SMEM(sinks.shape, f32),
        v(sgain.shape, f32), v(wgain.shape, f32), v(post_gain.shape, f32),
        v((2, rows, feat_half), bf), v((2, heads, 128), f32), v((rows, feats), bf),
        v(wqs.shape, bf), v(wks.shape, bf), v(wvs.shape, bf), v(wqw.shape, bf), v(wkw.shape, bf),
        v(wvw.shape, bf), v(wos.shape, bf), v(wow.shape, bf),
        v((heads, 2, half + half // 2, wide), bf), v((n_sp, 2, half + half // 2, wide), bf),
        v((n_sp * half, wide), bf), v((4 * half, n_sp * rows), f32),
        v((rows, kvw_cols), bf), v((rows, kvw_cols), bf), v((rows, sw), bf),
        v((n_sp, half // 2, wide), bf), v((heads, 2, half // 2, wide), bf), v((rows, sw), f32),
        v((2, rows, 128), f32), v((2, rows, 128), f32), v((rows, feats), f32), v((rows, feats), f32),
        v((n_cut, half, feats // n_cut), bf), v((n_cut, half, feats // n_cut), bf),
        dma((14,)), dma, dma, dma, dma, dma, dma((heads, 2)), dma((n_sp,)),
        dma((n_sp,)), dma((n_sp,)), dma, dma, dma((n_sp,)), dma((heads, 2)), dma((2,)), dma((2,)),
        dma((n_cut,)), dma((n_cut,)),
    ]
    return pl.pallas_call(
        functools.partial(kernel, n_sp),
        out_shape=jax.ShapeDtypeStruct((half, feats), bf),
        in_specs=[anywhere] * len(args),
        out_specs=vmem,
        scratch_shapes=scratch,
        compiler_params=pltpu.CompilerParams(
            collective_id=0, has_side_effects=True, vmem_limit_bytes=67043328
        ),
        name="layer",
    )(*args)


def passed_along(value, axis, steps):
    count = lax.axis_size(axis)
    initial, last = (max(0, -steps), min(count, count - steps))
    return lax.ppermute(value, axis, [(source, source + steps) for source in range(initial, last)])


def rounded(values):
    return lax.optimization_barrier(values.astype(jnp.bfloat16)).astype(jnp.float32)


def norm_rows(values, gain):
    stats = jnp.mean(values * values, axis=-1, keepdims=True)
    return values * lax.rsqrt(stats + EPS) * gain


def stick_block(queries, key_pair, head_bias, key_mask, carried):
    result, logsum = carried
    head_count = queries.shape[1]
    key_rows = key_pair[0].reshape(key_pair.shape[1], head_count, HEAD_DIM)
    values = key_pair[1].reshape(key_pair.shape[1], head_count, HEAD_DIM)
    scores = jnp.einsum(
        "thd,shd->hts", queries, key_rows, preferred_element_type=jnp.float32
    ) * HEAD_DIM ** (-0.5)
    scores = scores + head_bias[:, None, None]
    usable = key_mask[None]
    log_keep = jnp.where(usable, jax.nn.log_sigmoid(-scores), 0.0)
    suffix = lax.cumsum(log_keep, axis=2, reverse=True) - log_keep
    stick_weights = jnp.where(
        usable, jnp.exp(jax.nn.log_sigmoid(scores) + suffix + logsum[:, :, None]), 0.0
    )
    stick_weights = stick_weights.astype(jnp.bfloat16)
    result = result + jnp.einsum(
        "hts,shd->htd", stick_weights, values, preferred_element_type=jnp.float32
    )
    logsum = logsum + jnp.sum(log_keep, axis=2)
    return (result, logsum)


def by_collectives(
    tokens,
    pre_gain,
    w_query_stick,
    w_key_stick,
    w_value_stick,
    w_query_window,
    w_key_window,
    w_value_window,
    stick_bias,
    sinks,
    stick_gain,
    window_gain,
    w_out_stick,
    w_out_window,
    post_gain,
):
    gathered = lax.all_gather(tokens, "tp", axis=1, tiled=True)
    normed = norm_rows(gathered.astype(jnp.float32), pre_gain).astype(jnp.bfloat16)

    def project(weight):
        return jnp.dot(normed, weight, preferred_element_type=jnp.float32).astype(jnp.bfloat16)

    tok_rows = normed.shape[0]
    dev_index = lax.axis_index("sp")
    dev_count = lax.axis_size("sp")
    query_stick = project(w_query_stick)
    stick_heads = query_stick.shape[1] // HEAD_DIM
    queries = query_stick.reshape(tok_rows, stick_heads, HEAD_DIM)
    own_pair = jnp.stack([project(w_key_stick), project(w_value_stick)])
    pair_width = own_pair.shape[2]
    positions = jnp.arange(tok_rows, dtype=jnp.int32)
    initial = (
        jnp.zeros((stick_heads, tok_rows, HEAD_DIM), jnp.float32),
        jnp.zeros((stick_heads, tok_rows), jnp.float32),
    )
    collected = own_pair[None]
    for section_index in range(dev_count.bit_length() - 1):
        arrived = passed_along(collected, "sp", 2**section_index)
        collected = jnp.concatenate([arrived, collected], axis=0)
    per_group = min(dev_count, 8)
    group_count = dev_count // per_group
    grouped = collected.reshape(group_count, per_group, 2, tok_rows, pair_width)
    grouped = grouped.transpose(0, 2, 1, 3, 4).reshape(
        group_count, 2, per_group * tok_rows, pair_width
    )
    first_source = dev_index - (dev_count - 1)
    group_starts = (first_source + jnp.arange(group_count, dtype=jnp.int32) * per_group) * tok_rows
    query_pos = dev_index * tok_rows + positions
    span_offs = jnp.arange(per_group * tok_rows, dtype=jnp.int32)

    def visit_group(carried, inputs):
        key_pair, start_pos = inputs
        key_pos = start_pos + span_offs
        key_mask = (key_pos[None, :] >= 0) & (key_pos[None, :] < query_pos[:, None])
        return (stick_block(queries, key_pair, stick_bias, key_mask, carried), None)

    (stick_sum, _), _ = lax.scan(visit_group, initial, (grouped, group_starts), reverse=True)
    stick_out = (
        stick_sum.transpose(1, 0, 2).reshape(tok_rows, stick_heads * HEAD_DIM).astype(jnp.bfloat16)
    )
    query_window = project(w_query_window)
    window_pair = jnp.stack([project(w_key_window), project(w_value_window)])
    kv_heads = window_pair.shape[2] // HEAD_DIM
    previous = passed_along(window_pair, "sp", 1)
    extended = jnp.concatenate([previous, window_pair], axis=1)
    block_count = tok_rows // WINDOW
    extended = extended.reshape(2, block_count + 1, WINDOW, kv_heads, HEAD_DIM)
    banded = jnp.concatenate([extended[:, :-1], extended[:, 1:]], axis=2)
    q_blocks = query_window.reshape(block_count, WINDOW, kv_heads, GROUP, HEAD_DIM)
    logits = jnp.einsum(
        "nqhgd,nchd->nhgqc", q_blocks, banded[0], preferred_element_type=jnp.float32
    ) * HEAD_DIM ** (-0.5)
    query_offs = jnp.arange(WINDOW, dtype=jnp.int32)[:, None]
    key_offs = jnp.arange(2 * WINDOW, dtype=jnp.int32)[None, :]
    distance = query_offs + WINDOW - key_offs
    key_pos = (
        dev_index * tok_rows
        + jnp.arange(block_count, dtype=jnp.int32)[:, None] * WINDOW
        - WINDOW
        + key_offs
    )
    usable = ((distance >= 0) & (distance < WINDOW))[None] & (key_pos >= 0)[:, None, :]
    logits = jnp.where(usable[:, None, None], logits, -jnp.inf)
    sink_logit = sinks.reshape(kv_heads, GROUP)[None, :, :, None, None]
    row_top = jnp.maximum(jnp.max(logits, axis=-1, keepdims=True), sink_logit)
    weights_exp = jnp.exp(logits - row_top)
    normalizer = jnp.sum(weights_exp, axis=-1, keepdims=True) + jnp.exp(sink_logit - row_top)
    window_weights = (weights_exp / normalizer).astype(jnp.bfloat16)
    window_sum = jnp.einsum(
        "nhgqc,nchd->nqhgd", window_weights, banded[1], preferred_element_type=jnp.float32
    )
    window_out = window_sum.reshape(tok_rows, query_window.shape[1]).astype(jnp.bfloat16)
    stick_float = stick_out.astype(jnp.float32)
    window_float = window_out.astype(jnp.float32)
    squares = lax.psum(
        (jnp.sum(stick_float * stick_float, axis=1), jnp.sum(window_float * window_float, axis=1)),
        "tp",
    )
    stick_normed = (
        stick_float * lax.rsqrt(squares[0][:, None] / (stick_gain.shape[0] * lax.axis_size("tp")) + EPS) * stick_gain
    ).astype(jnp.bfloat16)
    window_normed = (
        window_float * lax.rsqrt(squares[1][:, None] / (window_gain.shape[0] * lax.axis_size("tp")) + EPS) * window_gain
    ).astype(jnp.bfloat16)
    total = jnp.dot(stick_normed, w_out_stick, preferred_element_type=jnp.float32)
    combined = lax.psum_scatter(
        (total + jnp.dot(window_normed, w_out_window, preferred_element_type=jnp.float32)).astype(
            jnp.bfloat16
        ),
        "tp",
        scatter_dimension=0,
        tiled=True,
    ).astype(jnp.float32)
    combined = rounded(combined)
    return norm_rows(combined, post_gain).astype(jnp.bfloat16)


def solution(mesh):
    in_specs = (
        P("sp", "tp"),
        P(),
        P(None, "tp"),
        P(None, "tp"),
        P(None, "tp"),
        P(None, "tp"),
        P(None, "tp"),
        P(None, "tp"),
        P("tp"),
        P("tp"),
        P("tp"),
        P("tp"),
        P("tp", None),
        P("tp", None),
        P(),
    )
    n_sp, n_tp = mesh.shape["sp"], mesh.shape["tp"]

    def shards(*args):
        heads = args[2].shape[1] // HEAD_DIM
        if n_tp == 2 and n_tp * heads == n_sp and args[0].shape[0] == WINDOW and n_sp % 4 == 0:
            return one_kernel(n_sp, *args)
        return by_collectives(*args)

    return jax.shard_map(
        shards,
        mesh=mesh,
        in_specs=in_specs,
        out_specs=P(("sp", "tp"), None),
        check_vma=False,
    )
```
